128 devices in a mesh: sp: 16 (over z, y), tp: 8 (over x, core).
Axes of the slice: x: 4, y: 4, z: 4, core: 2. Of those that a mesh axis runs over, the one named last changes fastest.
Arguments:
- arriving_hidden_sum: bfloat16 [16384, 2048], P('sp'), may hold values from -40 to 40
- content_entries_clustered: bfloat16 [16384, 4096], P('sp', 'tp'), may hold values from -6 to 6
- leaving_switch_entries: bfloat16 [16384, 4096], P('sp', 'tp'), may hold values from -6 to 6
- linked_source_target_pairs: bfloat16 [16384, 8, 2, 128], P('sp', 'tp'), may hold values from -1.78125 to 1.78125
- raw_interval_length: bfloat16 [16384, 64], P('sp', 'tp'), may hold values from -5 to 5
- spike_extra_lognoise: float32 [16384, 64], P('sp', 'tp'), may hold values from -0.6 to 0
- content_filter_kernel: bfloat16 [4, 4096], P(None, 'tp'), may hold values from -3 to 3
- coupling_filter_kernel: bfloat16 [4, 8, 2, 128], P(None, 'tp'), may hold values from -3 to 3
- interval_shift_vector: float32 [64], P('tp'), may hold values from -0.5 to 0.5
- fading_speed_exponent: float32 [64], P('tp'), may hold values from -16 to -2.9
- skip_channel_factor: float32 [64], P('tp'), may hold values from 1 to 10
- cluster_rescale_vector: float32 [4096], P('tp'), may hold values from 0.1 to 1.9
- blender_final_tensor: bfloat16 [4096, 2048], P('tp'), may hold values from -0.09375 to 0.09375
- prelayer_rescale_vector: float32 [2048], replicated, may hold values from 0.1 to 1.9
- switching_linear_tensor: bfloat16 [2048, 5632], P('sp', 'tp'), may hold values from -0.125 to 0.125
- widening_linear_tensor: bfloat16 [2048, 5632], P('sp', 'tp'), may hold values from -0.125 to 0.125
- contracting_linear_tensor: bfloat16 [5632, 2048], P('tp', 'sp'), may hold values from -0.078125 to 0.078125
Outputs:
- residual_out: bfloat16 [16384, 2048], P('sp', 'tp')
The draws below stay inside these ranges and needn't reach their ends.
All inputs are finite; a program needn't handle non-finite values.
Results may differ from the reference program's by a relative error of at most 0.012.
Values may be sent and summed in bfloat16 or wider, within the bound.
No kernel may reach another device: no remote copies, remote signals or barrier semaphores. Data moves between devices by JAX's collectives and lax.ppermute only.
A program may use at most 128 MiB of HBM per device.

```python
import math
import jax
import jax.numpy as jnp
from jax import lax

D = 2048
HEADS = 64
HEAD_DIM = 64
GROUPS = 8
STATE = 128
FF = 5632
CONV = 4
BLOCK_POSITIONS = 128
TOK_DEV = 1024
DI = 4096
TOKENS = 16384
N_TP = 8


def draw_arriving_hidden_sum(key, part):
    noise_key = jax.random.fold_in(key, 11)
    col_key = jax.random.fold_in(key, 12)
    row_key = jax.random.fold_in(key, 13)
    columns = jnp.arange(D, dtype=jnp.float32) / D
    row_scale = jnp.exp(jax.random.uniform(row_key, (TOKENS, 1), jnp.float32, jnp.log(0.4), jnp.log(4.0)))
    base = jnp.clip(jax.random.normal(noise_key, (TOKENS, D), jnp.float32), -6.0, 6.0)
    col_scale = 12.0 ** columns * jnp.exp(jax.random.uniform(col_key, (D,), jnp.float32, -0.35, 0.35))
    return jnp.clip(0.2 * base * row_scale * col_scale, -40.0, 40.0).astype(jnp.bfloat16)


def draw_raw_interval_length(key, part):
    noise_key = jax.random.fold_in(key, 21)
    shift_key = jax.random.fold_in(key, 22)
    shifts = jax.random.uniform(shift_key, (TOKENS // TOK_DEV, 1, 1), jnp.float32, -1.0, 1.0)
    noise = jnp.clip(0.7 * jax.random.normal(noise_key, (TOKENS // TOK_DEV, TOK_DEV, HEADS), jnp.float32), -4.0, 4.0)
    return (noise + shifts).reshape(TOKENS, HEADS).astype(jnp.bfloat16)


def draw_spike_extra_lognoise(key, part):
    spot_key = jax.random.fold_in(key, 31)
    loss_key = jax.random.fold_in(key, 32)
    spots = jax.random.randint(spot_key, (3,), 0, TOKENS)
    losses = jnp.log(jax.random.uniform(loss_key, (3, HEADS), jnp.float32, 0.55, 0.8))
    return jnp.zeros((TOKENS, HEADS), jnp.float32).at[spots].add(losses)


def draw_fading_speed_exponent(key, part):
    pick_key = jax.random.fold_in(key, 41)
    fast_key = jax.random.fold_in(key, 42)
    slow_key = jax.random.fold_in(key, 43)
    share = 0.5
    fast_pick = jax.random.uniform(pick_key, (HEADS,), jnp.float32) < share
    fast_rate = jax.random.uniform(fast_key, (HEADS,), jnp.float32, jnp.log(0.015), jnp.log(0.05))
    slow_rate = jax.random.uniform(slow_key, (HEADS,), jnp.float32, jnp.log(0.15), jnp.log(0.5)) - jnp.log(1.0 * TOKENS)
    return jnp.where(fast_pick, fast_rate, slow_rate)


def steps_of(own_key, shape, cuts, low, largest):
    loudness, own = 1.0, jax.random.fold_in(own_key, 6)
    for dim, parts in cuts:
        heights = jnp.exp(jax.random.uniform(jax.random.fold_in(own, dim), (parts,), jnp.float32, low / len(cuts), largest / len(cuts)))
        loudness = loudness * jnp.repeat(heights, shape[dim] // parts).reshape([-1 if axis == dim else 1 for axis in range(len(shape))])
    return loudness


def centred(key, dims, spread, most, split=(), kind=jnp.bfloat16):
    drawn = spread * jax.random.normal(key, dims, jnp.float32)
    if split:
        drawn = drawn * steps_of(key, dims, split, -0.22, 0.18)
    return jnp.clip(drawn, -most, most).astype(kind)


def setup_inputs(seed: int = 0) -> dict:
    streams_of = jax.random.split(jax.random.key(seed), 18)
    return {
        "arriving_hidden_sum": draw_arriving_hidden_sum(jax.random.fold_in(streams_of[17], 71), 0),
        "content_entries_clustered": centred(streams_of[1], (TOKENS, DI), 1.0, 6.0, ((0, 16), (1, 8))),
        "leaving_switch_entries": centred(streams_of[2], (TOKENS, DI), 1.0, 6.0, ((0, 16), (1, 8))),
        "linked_source_target_pairs": centred(streams_of[3], (TOKENS, GROUPS, 2, STATE), (STATE ** -0.25), 1.78125, ((0, 16), (1, 8))),
        "raw_interval_length": draw_raw_interval_length(jax.random.fold_in(streams_of[17], 71), 0),
        "spike_extra_lognoise": draw_spike_extra_lognoise(jax.random.fold_in(streams_of[17], 71), 0),
        "content_filter_kernel": centred(streams_of[6], (CONV, DI), CONV ** -0.5, 3.0, ((1, 8),)),
        "coupling_filter_kernel": centred(streams_of[7], (CONV, GROUPS, 2, STATE), CONV ** -0.5, 3.0, ((1, 8),)),
        "interval_shift_vector": jnp.clip(jax.random.uniform(streams_of[8], (HEADS,), jnp.float32, -0.5, 0.5) * steps_of(streams_of[8], (HEADS,), ((0, 8),), -0.4, 0.0), -0.5, 0.5),
        "fading_speed_exponent": draw_fading_speed_exponent(jax.random.fold_in(streams_of[17], 71), 0),
        "skip_channel_factor": jnp.clip(jnp.exp(math.log(10.0) - 2.3025851 * jax.random.uniform(streams_of[10], (HEADS,), jnp.float32) ** steps_of(streams_of[10], (HEADS,), ((0, 8),), -0.2, 0.2)), 1.0, 10.0),
        "cluster_rescale_vector": jnp.clip(1.0 + 0.18 * jax.random.normal(streams_of[11], (DI,), jnp.float32), 0.1, 1.9),
        "blender_final_tensor": centred(streams_of[12], (DI, D), DI ** -0.5, 0.09375, ((0, 8),)),
        "prelayer_rescale_vector": jnp.clip(1.0 + 0.18 * jax.random.normal(streams_of[13], (D,), jnp.float32), 0.1, 1.9),
        "switching_linear_tensor": centred(streams_of[14], (D, FF), D ** -0.5, 0.125, ((0, 16), (1, 8))),
        "widening_linear_tensor": centred(streams_of[15], (D, FF), D ** -0.5, 0.125, ((0, 16), (1, 8))),
        "contracting_linear_tensor": centred(streams_of[16], (FF, D), FF ** -0.5, 0.078125, ((0, 8), (1, 16))),
    }


EPS = 1e-06
highest = lax.Precision.HIGHEST

def causal_conv(values, taps):
    taps_count = taps.shape[0]
    length = values.shape[0]
    padded = jnp.pad(values.astype(jnp.float32), ((taps_count - 1, 0), (0, 0)))
    running = jnp.zeros(values.shape, jnp.float32)
    for tap_index in range(taps_count):
        running = running + padded[tap_index:tap_index + length] * taps[tap_index].astype(jnp.float32)
    return jax.nn.silu(running).astype(jnp.bfloat16)

def reference(arriving_hidden_sum, content_entries_clustered, leaving_switch_entries, linked_source_target_pairs, raw_interval_length, spike_extra_lognoise, content_filter_kernel, coupling_filter_kernel, interval_shift_vector, fading_speed_exponent, skip_channel_factor, cluster_rescale_vector, blender_final_tensor, prelayer_rescale_vector, switching_linear_tensor, widening_linear_tensor, contracting_linear_tensor):
    length = content_entries_clustered.shape[0]
    per_group = HEADS // GROUPS
    block_count = length // BLOCK_POSITIONS
    values = causal_conv(content_entries_clustered, content_filter_kernel)
    maps = causal_conv(linked_source_target_pairs.reshape(length, -1), coupling_filter_kernel.reshape(CONV, -1)).reshape(length, GROUPS, 2, STATE)
    write_map = maps[:, :, 0]
    read_map = maps[:, :, 1]
    interval_lengths = jax.nn.softplus(raw_interval_length.astype(jnp.float32) + interval_shift_vector)
    fading_log_factor = -jnp.exp(fading_speed_exponent) * interval_lengths + spike_extra_lognoise
    causal = jnp.tril(jnp.ones((BLOCK_POSITIONS, BLOCK_POSITIONS), bool))

    def block_step(carry_state, inputs):
        value_block, write_block, read_block, step_block, log_block = inputs
        cum_log = jnp.cumsum(log_block, axis=0)
        head_cum = cum_log.T
        log_gap = head_cum[:, :, None] - head_cum[:, None, :]
        intersection = jnp.einsum('lgn,sgn->gls', read_block.astype(jnp.float32), write_block.astype(jnp.float32))
        intersection = jnp.repeat(intersection, per_group, axis=0)
        weights = (intersection * jnp.exp(jnp.where(causal, log_gap, -jnp.inf)) * step_block.T[:, None, :]).astype(jnp.bfloat16)
        within = jnp.einsum('hls,shp->lhp', weights.astype(jnp.float32), value_block.astype(jnp.float32))
        carried = jnp.einsum('lgn,grpn->lgrp', read_block.astype(jnp.float32), carry_state, precision=highest)
        carried = carried.reshape(BLOCK_POSITIONS, HEADS, HEAD_DIM) * jnp.exp(cum_log)[:, :, None]
        end_log = cum_log[-1]
        scaled = (value_block.astype(jnp.float32) * (step_block * jnp.exp(end_log[None, :] - cum_log))[:, :, None]).astype(jnp.bfloat16)
        block_states = jnp.einsum('lgn,lgrp->grpn', write_block.astype(jnp.float32), scaled.astype(jnp.float32).reshape(BLOCK_POSITIONS, GROUPS, per_group, HEAD_DIM))
        carry_state = carry_state * jnp.exp(end_log).reshape(GROUPS, per_group)[:, :, None, None] + block_states
        return (carry_state, within + carried)
    value_heads = values.reshape(length, HEADS, HEAD_DIM)
    inputs = (value_heads.reshape(block_count, BLOCK_POSITIONS, HEADS, HEAD_DIM), write_map.reshape(block_count, BLOCK_POSITIONS, GROUPS, STATE), read_map.reshape(block_count, BLOCK_POSITIONS, GROUPS, STATE), interval_lengths.reshape(block_count, BLOCK_POSITIONS, HEADS), fading_log_factor.reshape(block_count, BLOCK_POSITIONS, HEADS))
    start_state = jnp.zeros((GROUPS, per_group, HEAD_DIM, STATE), jnp.float32)
    _, mixer = lax.scan(block_step, start_state, inputs)
    mixer = mixer.reshape(length, HEADS, HEAD_DIM) + value_heads.astype(jnp.float32) * skip_channel_factor[None, :, None]
    gated = mixer.reshape(length, DI) * jax.nn.silu(leaving_switch_entries.astype(jnp.float32))
    grouped = gated.reshape(length, GROUPS, DI // GROUPS)
    grouped = grouped * lax.rsqrt(lax.optimization_barrier(jnp.mean(grouped * grouped, axis=-1, keepdims=True)) + EPS)
    mixed_rows = (grouped.reshape(length, DI) * cluster_rescale_vector).astype(jnp.bfloat16)
    part_width = DI // N_TP
    mixer_out = jnp.zeros((length, D), jnp.float32)
    for device_rank in range(N_TP):
        partial_sum = jnp.dot(mixed_rows[:, device_rank * part_width:(device_rank + 1) * part_width], blender_final_tensor[device_rank * part_width:(device_rank + 1) * part_width], preferred_element_type=jnp.float32)
        mixer_out = mixer_out + lax.optimization_barrier(partial_sum.astype(jnp.bfloat16)).astype(jnp.float32)
    residual_mid = (arriving_hidden_sum.astype(jnp.float32) + mixer_out).astype(jnp.bfloat16)
    squares = residual_mid.astype(jnp.float32)
    normed = (squares * lax.rsqrt(lax.optimization_barrier(jnp.mean(squares * squares, axis=-1, keepdims=True)) + EPS) * prelayer_rescale_vector).astype(jnp.bfloat16)
    gate_pre = jnp.dot(normed, switching_linear_tensor, preferred_element_type=jnp.float32)
    up_pre = jnp.dot(normed, widening_linear_tensor, preferred_element_type=jnp.float32)
    hidden = (jax.nn.silu(gate_pre) * up_pre).astype(jnp.bfloat16)
    hidden_width = FF // N_TP
    mlp_out = jnp.zeros((length, D), jnp.float32)
    for device_rank in range(N_TP):
        partial_sum = jnp.dot(hidden[:, device_rank * hidden_width:(device_rank + 1) * hidden_width], contracting_linear_tensor[device_rank * hidden_width:(device_rank + 1) * hidden_width], preferred_element_type=jnp.float32)
        mlp_out = mlp_out + lax.optimization_barrier(partial_sum.astype(jnp.bfloat16)).astype(jnp.float32)
    return (residual_mid.astype(jnp.float32) + 0.5 * mlp_out).astype(jnp.bfloat16)
```

```python
import jax
import jax.numpy as jnp
from jax import lax
from jax.experimental import pallas as pl
from jax.experimental.pallas import tpu as pltpu
from jax.sharding import Mesh
from jax.sharding import PartitionSpec as P

BF = jnp.bfloat16
F32 = jnp.float32
EPS = 1e-06
T = 1024
BLK = 128
NB = T // BLK
HEADS = 8
CH = 512
ST = 128
PAIR = 128
HALO = 16
LOGROWS = 16
D = 2048
COL = 256
FF = 704
PACK = 2 * FF + FF
CHUNKS = 1
TC = T // CHUNKS

SP = ("z", "y")

VMEM = pl.BlockSpec(memory_space=pltpu.VMEM)
SMEM = pl.BlockSpec(memory_space=pltpu.SMEM)
ANY = pl.BlockSpec(memory_space=pl.ANY)


def sds(shape, kind):
    return jax.ShapeDtypeStruct(shape, kind)


def params(mib=48):
    return pltpu.CompilerParams(vmem_limit_bytes=mib * 1024 * 1024)


def silu(x):
    return x * jax.nn.sigmoid(x)


def hi_dot(a, b):
    return jnp.dot(a, b, preferred_element_type=F32, precision=lax.Precision.HIGHEST)


def lane_low():
    return lax.broadcasted_iota(jnp.int32, (1, PAIR), 1) < PAIR // 2


def widen(cols):
    low = lane_low()
    parts = [
        jnp.where(low, cols[:, 2 * p : 2 * p + 1], cols[:, 2 * p + 1 : 2 * p + 2])
        for p in range(HEADS // 2)
    ]
    return jnp.concatenate(parts, axis=1)


def conv_rows(ext, taps):
    total = ext[HALO - 3 : HALO - 3 + BLK] * taps[0:1]
    for k in range(1, 4):
        total = total + ext[HALO - 3 + k : HALO - 3 + k + BLK] * taps[k : k + 1]
    return silu(total).astype(BF)


def state_body(
    content, pairs, halo, step, log, taps_c, taps_p,
    values, maps, cum_out, entering, payload,
    ext_c, ext_p, carry, prior,
):
    ext_c[0:HALO] = halo[:, 0:CH]
    ext_p[0:HALO] = halo[:, CH : CH + 256]
    ext_c[HALO : HALO + T] = content[...]
    ext_p[HALO : HALO + T] = pairs[...]
    carry[...] = jnp.zeros((ST, CH), F32)
    prior[...] = jnp.zeros((8, HEADS), F32)
    row = lax.broadcasted_iota(jnp.int32, (BLK, BLK), 0)
    col = lax.broadcasted_iota(jnp.int32, (BLK, BLK), 1)
    tril = (col <= row).astype(F32)
    tc = taps_c[...].astype(F32)
    tp = taps_p[...].astype(F32)

    def block(b, _):
        at = pl.multiple_of(b * BLK, BLK)
        rows = pl.ds(at, BLK)
        wide = pl.ds(at, BLK + HALO)
        v = conv_rows(ext_c[wide, :].astype(F32), tc)
        m = conv_rows(ext_p[wide, :].astype(F32), tp)
        values[rows, :] = v
        maps[rows, :] = m
        cum = hi_dot(tril, log[rows, :])
        end = cum[BLK - 1 : BLK, :]
        before = prior[0:1, :]
        cum_out[rows, :] = cum + before
        prior[...] = jnp.broadcast_to(before + end, (8, HEADS))
        factor = step[rows, :] * jnp.exp(end - cum)
        scaled = (v.astype(F32) * widen(factor)).astype(BF)
        added = lax.dot_general(
            m[:, 0:ST], scaled, (((0,), (0,)), ((), ())), preferred_element_type=F32
        )
        old = carry[...]
        entering[b] = old.astype(BF)
        carry[...] = old * widen(jnp.exp(end)) + added
        return 0

    lax.fori_loop(0, NB, block, 0)
    payload[0:ST, :] = carry[...].astype(BF)
    total = widen(prior[...])
    high = total.astype(BF)
    low = (total - high.astype(F32)).astype(BF)
    payload[ST : ST + LOGROWS, :] = jnp.concatenate([high, low], axis=0)


def state_kernel(content, pairs, halo, step, log, taps_c, taps_p):
    return pl.pallas_call(
        state_body,
        out_shape=(
            sds((T, CH), BF),
            sds((T, 256), BF),
            sds((T, HEADS), F32),
            sds((NB, ST, CH), BF),
            sds((ST + LOGROWS, CH), BF),
        ),
        in_specs=[VMEM] * 7,
        out_specs=(VMEM,) * 5,
        scratch_shapes=[
            pltpu.VMEM((T + HALO, CH), BF),
            pltpu.VMEM((T + HALO, 256), BF),
            pltpu.VMEM((ST, CH), F32),
            pltpu.VMEM((8, HEADS), F32),
        ],
        compiler_params=params(),
        name="state",
    )(content, pairs, halo, step, log, taps_c, taps_p)


def local_body(values, maps, log, log_t, step_t, entering, skip, out):
    row = lax.broadcasted_iota(jnp.int32, (BLK, BLK), 0)
    col = lax.broadcasted_iota(jnp.int32, (BLK, BLK), 1)
    causal = col <= row
    tril = causal.astype(F32)
    triu = (row <= col).astype(F32)
    low = lane_low()
    gain = widen(skip[...])

    def block(b, _):
        at = pl.multiple_of(b * BLK, BLK)
        rows = pl.ds(at, BLK)
        v = values[rows, :]
        m = maps[rows, :]
        write, read = m[:, 0:ST], m[:, ST : 2 * ST]
        cum = hi_dot(tril, log[rows, :])
        cum_t = hi_dot(log_t[b], triu)
        steps = step_t[b]
        meet = lax.dot_general(
            read, write, (((1,), (1,)), ((), ())), preferred_element_type=F32
        )
        parts = []
        for p in range(HEADS // 2):
            weights = []
            for h in (2 * p, 2 * p + 1):
                gap = cum[:, h : h + 1] - cum_t[h : h + 1, :]
                decay = jnp.exp(jnp.where(causal, gap, -jnp.inf))
                weights.append((meet * decay * steps[h : h + 1, :]).astype(BF))
            vp = v[:, p * PAIR : (p + 1) * PAIR]
            none = jnp.zeros_like(vp)
            stacked = jnp.concatenate(
                [jnp.where(low, vp, none), jnp.where(low, none, vp)], axis=0
            )
            parts.append(
                jnp.dot(
                    jnp.concatenate(weights, axis=1), stacked, preferred_element_type=F32
                )
            )
        within = jnp.concatenate(parts, axis=1)
        carried = jnp.dot(read, entering[b], preferred_element_type=F32)
        out[rows, :] = within + carried * widen(jnp.exp(cum)) + v.astype(F32) * gain
        return 0

    lax.fori_loop(0, NB, block, 0)


def local_kernel(values, maps, log, log_t, step_t, entering, skip):
    return pl.pallas_call(
        local_body,
        out_shape=sds((T, CH), F32),
        in_specs=[VMEM] * 7,
        out_specs=VMEM,
        compiler_params=params(),
        cost_estimate=pl.CostEstimate(flops=6_000_000_000, transcendentals=0, bytes_accessed=6_000_000),
        name="local",
    )(values, maps, log, log_t, step_t, entering, skip)


def log_row(ref):
    return ref[ST : ST + 1, :].astype(F32) + ref[ST + 8 : ST + 9, :].astype(F32)


def scan_line(place, refs, state, prefix):
    state[...] = jnp.zeros((ST, CH), F32)
    prefix[...] = jnp.zeros((ST, CH), F32)
    count = len(refs)
    logs = [log_row(r) for r in refs]
    whole = jnp.zeros((1, CH), F32)
    ahead = jnp.zeros((1, CH), F32)
    for j in range(count):
        for d in range(count):

            @pl.when(lax.rem(place - j + count, count) == d)
            def _(d=d):
                if d == 0:
                    prefix[...] = state[...]
                state[...] = state[...] * jnp.exp(logs[d]) + refs[d][0:ST, :].astype(F32)

    for d in range(count):
        whole = whole + logs[d]
        ahead = ahead + jnp.where(place >= d, logs[d], 0.0) if d else ahead
    return whole, ahead


def line_body(place, r0, r1, r2, r3, payload, prefix, ahead_out, state):
    whole, ahead = scan_line(place[0], (r0, r1, r2, r3), state, prefix)
    payload[0:ST, :] = state[...].astype(BF)
    high = whole.astype(BF)
    low = (whole - high.astype(F32)).astype(BF)
    payload[ST : ST + 8, :] = jnp.broadcast_to(high, (8, CH))
    payload[ST + 8 : ST + 16, :] = jnp.broadcast_to(low, (8, CH))
    ahead_out[...] = jnp.broadcast_to(ahead, (8, CH))


def line_kernel(place, received):
    return pl.pallas_call(
        line_body,
        out_shape=(
            sds((ST + LOGROWS, CH), BF),
            sds((ST, CH), F32),
            sds((8, CH), F32),
        ),
        in_specs=[SMEM] + [VMEM] * 4,
        out_specs=(VMEM,) * 3,
        scratch_shapes=[pltpu.VMEM((ST, CH), F32)],
        compiler_params=params(),
        name="line",
    )(place, *received)


def mix_body(
    place, order, q0, q1, q2, q3, prefix, ahead, local, maps, cum, gate, gain, blend,
    send, keep, incoming, state, prefix_z, mixed,
):
    scan_line(place[0], (q0, q1, q2, q3), state, prefix_z)
    incoming[...] = (prefix_z[...] * jnp.exp(ahead[0:1, :]) + prefix[...]).astype(BF)
    rescale = gain[...]

    def block(b, _):
        rows = pl.ds(pl.multiple_of(b * BLK, BLK), BLK)
        read = maps[rows, ST : 2 * ST]
        arrived = jnp.dot(read, incoming[...], preferred_element_type=F32)
        mixer = local[rows, :] + arrived * widen(jnp.exp(cum[rows, :]))
        gated = mixer * silu(gate[rows, :].astype(F32))
        scale = lax.rsqrt(jnp.mean(gated * gated, axis=1, keepdims=True) + EPS)
        mixed[rows, :] = (gated * scale * rescale).astype(BF)
        return 0

    lax.fori_loop(0, NB, block, 0)
    for half, target in ((1, send), (0, keep)):
        for k in range(4):

            def project(b, _, half=half, k=k, target=target):
                rows = pl.ds(pl.multiple_of(b * 512, 512), 512)
                target[k, rows, :] = jnp.dot(
                    mixed[rows, :], blend[order[half * 4 + k]], preferred_element_type=F32
                ).astype(BF)
                return 0

            lax.fori_loop(0, T // 512, project, 0)


def mix_kernel(place, order, received, prefix, ahead, local, maps, cum, gate, gain, blend):
    return pl.pallas_call(
        mix_body,
        out_shape=(sds((4, T, COL), BF), sds((4, T, COL), BF)),
        in_specs=[SMEM] * 2 + [VMEM] * 12,
        out_specs=(VMEM,) * 2,
        scratch_shapes=[
            pltpu.VMEM((ST, CH), BF),
            pltpu.VMEM((ST, CH), F32),
            pltpu.VMEM((ST, CH), F32),
            pltpu.VMEM((T, CH), BF),
        ],
        compiler_params=params(),
        name="mix",
    )(place, order, *received, prefix, ahead, local, maps, cum, gate, gain, blend)


def ffn_body(
    order, pack, gain, m0, m1, m3, m2a, m2b, n0, n1, n3, n2a, n2b,
    send, keep, wide, narrow, rows_x, sems,
):
    def copies():
        for i in range(8):
            spot = order[i]
            for c in range(11):
                yield pltpu.make_async_copy(
                    pack.at[pl.ds(2 * spot, 2), pl.ds(c * 128, 128), :],
                    wide.at[pl.ds(2 * i, 2), :, pl.ds(c * 128, 128)],
                    sems.at[0],
                )

    def down():
        for i in range(8):
            spot = order[i]
            for j in range(2):
                yield pltpu.make_async_copy(
                    pack.at[2 * spot + j, pl.ds(2 * FF, FF), :],
                    narrow.at[i, :, pl.ds(j * 128, 128)],
                    sems.at[1],
                )

    for copy in copies():
        copy.start()
    for copy in down():
        copy.start()
    half = TC // 2
    pieces = (
        ((0, TC, m0),), ((0, TC, m1),), ((0, half, m2a), (half, half, m2b)), ((0, TC, m3),),
        ((0, TC, n0),), ((0, TC, n1),), ((0, half, n2a), (half, half, n2b)), ((0, TC, n3),),
    )
    total = jnp.zeros((TC, 1), F32)
    for i, piece in enumerate(pieces):
        x = jnp.concatenate([r[...] for _, _, r in piece], axis=0).astype(F32)
        total = total + jnp.sum(x * x, axis=1, keepdims=True)
    scale = lax.rsqrt(total * (1.0 / D) + EPS)
    for i, piece in enumerate(pieces):
        x = jnp.concatenate([r[...] for _, _, r in piece], axis=0).astype(F32)
        rows_x[:, i * COL : (i + 1) * COL] = (x * scale * gain[order[i]]).astype(BF)
    for copy in copies():
        copy.wait()
    for copy in down():
        copy.wait()
    step = 256

    def tile(b, _):
        rows = pl.ds(pl.multiple_of(b * step, step), step)
        both = jnp.dot(
            rows_x[rows, :], wide[...].reshape(D, 2 * FF), preferred_element_type=F32
        )
        hidden = (silu(both[:, :FF]) * both[:, FF:]).astype(BF)
        for i in range(8):
            target = keep if i < 4 else send
            target[i % 4, rows, :] = jnp.dot(
                hidden, narrow[i], preferred_element_type=F32
            ).astype(BF)
        return 0

    lax.fori_loop(0, TC // step, tile, 0)


def ffn_kernel(order, pack, gain, mine, theirs):
    return pl.pallas_call(
        ffn_body,
        out_shape=(sds((4, TC, COL), BF), sds((4, TC, COL), BF)),
        in_specs=[SMEM, ANY] + [VMEM] * 11,
        out_specs=(VMEM,) * 2,
        scratch_shapes=[
            pltpu.VMEM((16, 128, 2 * FF), BF),
            pltpu.VMEM((8, FF, COL), BF),
            pltpu.VMEM((TC, D), BF),
            pltpu.SemaphoreType.DMA((2,)),
        ],
        compiler_params=params(60),
        name="ffn",
    )(order, pack, gain, *mine, *theirs)


def turn(array, axis, distance):
    count = lax.axis_size(axis)
    return lax.ppermute(array, axis, [(i, (i + distance) % count) for i in range(count)])


def swap(array):
    return lax.ppermute(array, "c", [(0, 1), (1, 0)])


def reduce_parts(send, keep):
    got = swap(send)
    half = send.shape[1] // 2

    def chip(k, rows):
        return keep[k, rows].astype(F32) + got[k, rows].astype(F32)

    first, last = slice(None, half), slice(half, None)
    up = turn(jnp.concatenate([chip(2, first), chip(1, last)], 0).astype(BF), "x", 1)
    down = turn(jnp.concatenate([chip(3, first), chip(2, last)], 0).astype(BF), "x", -1)
    up_more = turn((chip(1, first) + up[:half].astype(F32)).astype(BF), "x", 1)
    down_more = turn((chip(3, last) + down[half:].astype(F32)).astype(BF), "x", -1)
    from_low = jnp.concatenate([up_more, up[half:]], 0).astype(F32)
    from_high = jnp.concatenate([down[:half], down_more], 0).astype(F32)
    return chip(0, slice(None)) + from_low + from_high


def gather_columns(own):
    half = own.shape[0] // 2
    below = turn(own, "x", 1)
    above = turn(own, "x", -1)
    far_a = turn(below[:half], "x", 1)
    far_b = turn(above[half:], "x", -1)
    mine = (own, below, above, far_a, far_b)
    return mine, tuple(swap(piece) for piece in mine)


def shards(
    arriving, content, gate, linked, raw, spike, taps_c, taps_p, shift, fading, skip,
    cluster_gain, blender, norm_gain, w_gate, w_up, w_down,
):
    x, c = lax.axis_index("x"), lax.axis_index("c")
    y, z = lax.axis_index("y"), lax.axis_index("z")
    both = jnp.concatenate([w_gate, w_up], axis=1).reshape(128, 11, 128)
    pack = jnp.concatenate([jnp.swapaxes(both, 0, 1).reshape(11 * 128, 128), w_down], axis=0)
    pack = lax.all_gather(pack, SP, axis=0, tiled=True).reshape(16, PACK, 128)
    pairs = linked.reshape(T, 256)
    tail = jnp.concatenate([content[T - HALO :], pairs[T - HALO :]], axis=1)
    halo = lax.ppermute(tail, SP, [(i, i + 1) for i in range(15)])
    step = jax.nn.softplus(raw.astype(F32) + shift)
    log = -jnp.exp(fading) * step + spike
    step_t = jnp.swapaxes(step.reshape(NB, BLK, HEADS), 1, 2)
    log_t = jnp.swapaxes(log.reshape(NB, BLK, HEADS), 1, 2)
    values, maps, cum, entering, payload = state_kernel(
        content, pairs, halo, step, log, taps_c, taps_p.reshape(4, 256)
    )
    line = [payload] + [turn(payload, "y", d) for d in (1, 2, 3)]
    local = local_kernel(
        values, maps, log, log_t, step_t, entering, skip.reshape(1, HEADS)
    )
    payload_z, prefix, ahead = line_kernel(y.reshape(1), line)
    lines = [payload_z] + [turn(payload_z, "z", d) for d in (1, 2, 3)]
    steps = jnp.arange(4, dtype=jnp.int32)
    chips = (x + steps) % 4
    order = jnp.concatenate([chips * 2 + c, chips * 2 + (1 - c)]).astype(jnp.int32)
    blend = jnp.swapaxes(blender.reshape(CH, 8, COL), 0, 1)
    send, keep = mix_kernel(
        z.reshape(1), order, lines, prefix, ahead, local, maps, cum, gate,
        cluster_gain.reshape(1, CH), blend,
    )
    mine_cols = lax.dynamic_slice_in_dim(arriving, (2 * x + c) * COL, COL, 1).astype(F32)
    back = (x - steps) % 4
    order_in = jnp.concatenate([back * 2 + c, back * 2 + (1 - c)]).astype(jnp.int32)
    del order_in
    outs = []
    for i in range(CHUNKS):
        rows = slice(i * TC, (i + 1) * TC)
        summed = reduce_parts(send[:, rows], keep[:, rows])
        own = (mine_cols[rows] + summed).astype(BF)
        mine, theirs = gather_columns(own)

        def arranged(piece):
            return (piece[0], piece[2], piece[1], piece[3], piece[4])

        send_f, keep_f = ffn_kernel(
            order, pack, norm_gain.reshape(8, 1, COL), arranged(mine), arranged(theirs)
        )
        mlp = reduce_parts(send_f, keep_f)
        outs.append((own.astype(F32) + 0.5 * mlp).astype(BF))
    return outs[0] if CHUNKS == 1 else jnp.concatenate(outs, axis=0)


def solution(mesh):
    torus = Mesh(mesh.devices.reshape(4, 4, 4, 2), ("z", "y", "x", "c"))
    tp = ("x", "c")
    return jax.shard_map(
        shards,
        mesh=torus,
        in_specs=(
            P(SP, None), P(SP, tp), P(SP, tp), P(SP, tp, None, None), P(SP, tp), P(SP, tp),
            P(None, tp), P(None, tp, None, None), P(tp), P(tp), P(tp), P(tp), P(tp, None),
            P(), P(SP, tp), P(SP, tp), P(tp, SP),
        ),
        out_specs=P(SP, tp),
        check_vma=False,
    )
```

```python
import functools

import jax
import jax.numpy as jnp
from jax import lax
from jax.experimental import pallas as pl
from jax.experimental.pallas import tpu as pltpu
from jax.sharding import Mesh
from jax.sharding import PartitionSpec as P


BF = jnp.bfloat16
F32 = jnp.float32
EPS = 1e-06
T = 1024
BLK = 128
NB = T // BLK
HEADS = 8
CH = 512
ST = 128
PAIR = 128
HALO = 16
LOGROWS = 16
D = 2048
COL = 256
FF = 704
PACK = 2 * FF + FF
FIRST = 512
SECOND = T - FIRST

SP = ("z", "y")

VMEM = pl.BlockSpec(memory_space=pltpu.VMEM)
SMEM = pl.BlockSpec(memory_space=pltpu.SMEM)
ANY = pl.BlockSpec(memory_space=pl.ANY)


def sds(shape, kind):
    return jax.ShapeDtypeStruct(shape, kind)


def params(mib=48):
    return pltpu.CompilerParams(vmem_limit_bytes=mib * 1024 * 1024)


def silu(x):
    return x * jax.nn.sigmoid(x)


def hi_dot(a, b):
    return jnp.dot(a, b, preferred_element_type=F32, precision=lax.Precision.HIGHEST)


def lane_low():
    return lax.broadcasted_iota(jnp.int32, (1, PAIR), 1) < PAIR // 2


def spread(rows, width, pieces):
    parts, rest = [], rows
    for _ in range(pieces):
        part = rest.astype(BF)
        rest = rest - part.astype(F32)
        parts.append(part)
    head = lax.broadcasted_iota(jnp.int32, (HEADS, HEADS * width), 0)
    lane = lax.broadcasted_iota(jnp.int32, (HEADS, HEADS * width), 1)
    ones = ((lane >= head * width) & (lane < (head + 1) * width)).astype(F32).astype(BF)
    return lax.dot_general(
        jnp.concatenate(parts, axis=0), jnp.concatenate([ones] * pieces, axis=0),
        (((0,), (0,)), ((), ())), preferred_element_type=F32,
    )


def block_lanes(b):
    return pl.ds(pl.multiple_of(b * BLK, BLK), BLK)


def conv_rows(ext, taps):
    total = ext[HALO - 3 : HALO - 3 + BLK] * taps[0:1]
    for k in range(1, 4):
        total = total + ext[HALO - 3 + k : HALO - 3 + k + BLK] * taps[k : k + 1]
    return silu(total).astype(BF)


def softplus(x):
    return jnp.maximum(x, 0.0) + jnp.log1p(jnp.exp(-jnp.abs(x)))


def state_body(
    content, pairs, halo, raw, spike, shift, fading, taps_c, taps_p,
    values, maps, cum_out, tot_out, step_out, entering, payload,
    ext_c, ext_p, factors, ends, carry,
):
    ext_c[0:HALO] = halo[:, 0:CH]
    ext_p[0:HALO] = halo[:, CH : CH + 256]
    ext_c[HALO : HALO + T] = content[...]
    ext_p[HALO : HALO + T] = pairs[...]
    carry[...] = jnp.zeros((ST, CH), F32)
    row = lax.broadcasted_iota(jnp.int32, (BLK, BLK), 0)
    col = lax.broadcasted_iota(jnp.int32, (BLK, BLK), 1)
    triu = (row <= col).astype(F32)
    tc = taps_c[...].astype(F32)
    tp = taps_p[...].astype(F32)
    step = softplus(raw[...].astype(F32) + shift[...])
    step_out[...] = step
    log = -jnp.exp(fading[...]) * step + spike[...]
    cum = hi_dot(
        jnp.concatenate([log[:, b * BLK : (b + 1) * BLK] for b in range(NB)], axis=0), triu
    )
    prior = jnp.zeros((HEADS, 1), F32)
    for b in range(NB):
        lanes = slice(b * BLK, (b + 1) * BLK)
        here = cum[b * HEADS : (b + 1) * HEADS]
        end = here[:, BLK - 1 : BLK]
        cum_out[:, lanes] = here
        tot_out[:, lanes] = here + prior
        factors[b] = step[:, lanes] * jnp.exp(end - here)
        ends[b] = jnp.broadcast_to(jnp.exp(end), (HEADS, BLK))
        prior = prior + end

    def block(b, _):
        at = pl.multiple_of(b * BLK, BLK)
        rows = pl.ds(at, BLK)
        wide = pl.ds(at, BLK + HALO)
        v = conv_rows(ext_c[wide, :].astype(F32), tc)
        m = conv_rows(ext_p[wide, :].astype(F32), tp)
        values[rows, :] = v
        maps[rows, :] = m
        scaled = (v.astype(F32) * spread(factors[b], 64, 2)).astype(BF)
        added = lax.dot_general(
            m[:, 0:ST], scaled, (((0,), (0,)), ((), ())), preferred_element_type=F32
        )
        old = carry[...]
        entering[b] = old.astype(BF)
        carry[...] = old * spread(ends[b], 64, 2) + added
        return 0

    lax.fori_loop(0, NB, block, 0, unroll=2)
    payload[0:ST, :] = carry[...].astype(BF)
    total = spread(jnp.broadcast_to(prior, (HEADS, BLK)), 64, 3)[0:8]
    high = total.astype(BF)
    low = (total - high.astype(F32)).astype(BF)
    payload[ST : ST + LOGROWS, :] = jnp.concatenate([high, low], axis=0)


def state_kernel(*args):
    return pl.pallas_call(
        state_body,
        out_shape=(
            sds((T, CH), BF),
            sds((T, 256), BF),
            sds((HEADS, T), F32),
            sds((HEADS, T), F32),
            sds((HEADS, T), F32),
            sds((NB, ST, CH), BF),
            sds((ST + LOGROWS, CH), BF),
        ),
        in_specs=[VMEM] * 9,
        out_specs=(VMEM,) * 7,
        scratch_shapes=[
            pltpu.VMEM((T + HALO, CH), BF),
            pltpu.VMEM((T + HALO, 256), BF),
            pltpu.VMEM((NB, HEADS, BLK), F32),
            pltpu.VMEM((NB, HEADS, BLK), F32),
            pltpu.VMEM((ST, CH), F32),
        ],
        compiler_params=params(16),
        name="state",
    )(*args)


def local_body(values, maps, cum_in, step_in, entering, skip, gate, blend, out, gate_out):
    row = lax.broadcasted_iota(jnp.int32, (BLK, BLK), 0)
    col = lax.broadcasted_iota(jnp.int32, (BLK, BLK), 1)
    causal = col <= row
    low = lane_low()
    gain = spread(jnp.broadcast_to(skip[...], (HEADS, BLK)), 64, 3)

    def block(b, _):
        rows = block_lanes(b)
        v = values[rows, :]
        m = maps[rows, :]
        write, read = m[:, 0:ST], m[:, ST : 2 * ST]
        cum = cum_in[:, rows]
        cum_wide = spread(cum, BLK, 3)
        steps = step_in[:, rows]
        meet = lax.dot_general(
            read, write, (((1,), (1,)), ((), ())), preferred_element_type=F32
        )
        parts = []
        for p in range(HEADS // 2):
            weights = []
            for h in (2 * p, 2 * p + 1):
                gap = cum_wide[:, h * BLK : (h + 1) * BLK] - cum[h : h + 1, :]
                decay = jnp.exp(jnp.where(causal, gap, -jnp.inf))
                weights.append((meet * decay * steps[h : h + 1, :]).astype(BF))
            vp = v[:, p * PAIR : (p + 1) * PAIR]
            none = jnp.zeros_like(vp)
            stacked = jnp.concatenate(
                [jnp.where(low, vp, none), jnp.where(low, none, vp)], axis=0
            )
            parts.append(
                jnp.dot(
                    jnp.concatenate(weights, axis=1), stacked, preferred_element_type=F32
                )
            )
        within = jnp.concatenate(parts, axis=1)
        carried = jnp.dot(read, entering[b], preferred_element_type=F32)
        carried = carried * spread(jnp.exp(cum), 64, 2)
        out[rows, :] = within + carried + v.astype(F32) * gain
        gate_out[rows, :] = silu(gate[rows, :].astype(F32))
        return 0

    lax.fori_loop(0, NB, block, 0)


def local_kernel(*args):
    return pl.pallas_call(
        local_body,
        out_shape=(sds((T, CH), F32), sds((T, CH), F32)),
        in_specs=[VMEM] * 8,
        out_specs=(VMEM,) * 2,
        compiler_params=params(12),
        cost_estimate=pl.CostEstimate(flops=6_000_000_000, transcendentals=0, bytes_accessed=6_000_000),
        name="local",
    )(*args)


def tail_body(content, pairs, out):
    out[:, 0:CH] = content[...]
    out[:, CH : CH + 256] = pairs[...]


def tail_kernel(content, pairs):
    last = T // HALO - 1
    return pl.pallas_call(
        tail_body,
        out_shape=sds((HALO, CH + 256), BF),
        grid=(1,),
        in_specs=[
            pl.BlockSpec((HALO, CH), lambda _: (last, 0)),
            pl.BlockSpec((HALO, 256), lambda _: (last, 0)),
        ],
        out_specs=VMEM,
        compiler_params=params(4),
        name="tail",
    )(content, pairs)


def log_row(ref):
    return ref[ST : ST + 1, :].astype(F32) + ref[ST + 8 : ST + 9, :].astype(F32)


def scan_line(place, refs, state, prefix):
    state[...] = jnp.zeros((ST, CH), F32)
    prefix[...] = jnp.zeros((ST, CH), F32)
    count = len(refs)
    logs = [log_row(r) for r in refs]
    whole = jnp.zeros((1, CH), F32)
    ahead = jnp.zeros((1, CH), F32)
    for j in range(count):
        for d in range(count):

            @pl.when(lax.rem(place - j + count, count) == d)
            def _(d=d):
                if d == 0:
                    prefix[...] = state[...]
                state[...] = state[...] * jnp.exp(logs[d]) + refs[d][0:ST, :].astype(F32)

    for d in range(count):
        whole = whole + logs[d]
        ahead = ahead + jnp.where(place >= d, logs[d], 0.0) if d else ahead
    return whole, ahead


def line_body(place, r0, r1, r2, r3, payload, prefix, ahead_out, state):
    whole, ahead = scan_line(place[0], (r0, r1, r2, r3), state, prefix)
    payload[0:ST, :] = state[...].astype(BF)
    high = whole.astype(BF)
    low = (whole - high.astype(F32)).astype(BF)
    payload[ST : ST + 8, :] = jnp.broadcast_to(high, (8, CH))
    payload[ST + 8 : ST + 16, :] = jnp.broadcast_to(low, (8, CH))
    ahead_out[...] = jnp.broadcast_to(ahead, (8, CH))


def line_kernel(place, received):
    return pl.pallas_call(
        line_body,
        out_shape=(
            sds((ST + LOGROWS, CH), BF),
            sds((ST, CH), F32),
            sds((8, CH), F32),
        ),
        in_specs=[SMEM] + [VMEM] * 4,
        out_specs=(VMEM,) * 3,
        scratch_shapes=[pltpu.VMEM((ST, CH), F32)],
        compiler_params=params(8),
        name="line",
    )(place, *received)


def incoming_body(place, q0, q1, q2, q3, prefix, ahead, incoming, state, prefix_z):
    scan_line(place[0], (q0, q1, q2, q3), state, prefix_z)
    incoming[...] = (prefix_z[...] * jnp.exp(ahead[0:1, :]) + prefix[...]).astype(BF)


def incoming_kernel(place, received, prefix, ahead):
    return pl.pallas_call(
        incoming_body,
        out_shape=sds((ST, CH), BF),
        in_specs=[SMEM] + [VMEM] * 6,
        out_specs=VMEM,
        scratch_shapes=[pltpu.VMEM((ST, CH), F32), pltpu.VMEM((ST, CH), F32)],
        compiler_params=params(8),
        name="incoming",
    )(place, *received, prefix, ahead)


def mix_body(
    start, count, order, incoming, local, maps, tot, gate, gain, blend, send, keep, mixed
):
    rescale = gain[...]

    def block(b, _):
        rows = pl.ds(pl.multiple_of(start + b * BLK, BLK), BLK)
        read = maps[rows, ST : 2 * ST]
        arrived = jnp.dot(read, incoming[...], preferred_element_type=F32)
        mixer = local[rows, :] + arrived * spread(jnp.exp(tot[:, rows]), 64, 2)
        gated = mixer * gate[rows, :]
        scale = lax.rsqrt(jnp.mean(gated * gated, axis=1, keepdims=True) + EPS)
        mixed[pl.ds(pl.multiple_of(b * BLK, BLK), BLK), :] = (gated * scale * rescale).astype(BF)
        return 0

    lax.fori_loop(0, count // BLK, block, 0, unroll=2)
    for half, target in ((1, send), (0, keep)):
        for k in range(4):
            cols = pl.ds(pl.multiple_of(order[half * 4 + k] * COL, COL), COL)
            target[k] = jnp.dot(
                mixed[...], blend[:, cols], preferred_element_type=F32
            ).astype(BF)


def mix_kernel(start, count, order, *args):
    return pl.pallas_call(
        functools.partial(mix_body, start, count),
        out_shape=(sds((4, count, COL), BF), sds((4, count, COL), BF)),
        in_specs=[SMEM] + [VMEM] * 7,
        out_specs=(VMEM,) * 2,
        scratch_shapes=[pltpu.VMEM((count, CH), BF)],
        compiler_params=params(16),
        cost_estimate=pl.CostEstimate(flops=3_000_000_000, transcendentals=0, bytes_accessed=6_000_000),
        name="mix",
    )(order, *args)


def pair_body(keep, got, c0, c1, c2, c3):
    for k, out in enumerate((c0, c1, c2, c3)):
        out[...] = (keep[k].astype(F32) + got[k].astype(F32)).astype(BF)


def pair_kernel(keep, got):
    count = keep.shape[1]
    return pl.pallas_call(
        pair_body,
        out_shape=(sds((count, COL), BF),) * 4,
        in_specs=[VMEM] * 2,
        out_specs=(VMEM,) * 4,
        compiler_params=params(8),
        name="pair",
    )(keep, got)


def total_of(refs):
    total = refs[0][...].astype(F32)
    for r in refs[1:]:
        total = total + r[...].astype(F32)
    return total


def own_body(start, c0, f1, f2, f3, arriving, out):
    count = out.shape[0]
    base = arriving[start : start + count, :].astype(F32)
    out[...] = (base + total_of((c0, f1, f2, f3))).astype(BF)


def own_kernel(start, parts, arriving):
    count = parts[0].shape[0]
    return pl.pallas_call(
        functools.partial(own_body, start),
        out_shape=sds((count, COL), BF),
        in_specs=[VMEM] * 5,
        out_specs=VMEM,
        compiler_params=params(8),
        name="own",
    )(*parts, arriving)


def last_body(own, c0, f1, f2, f3, out):
    out[...] = (own[...].astype(F32) + 0.5 * total_of((c0, f1, f2, f3))).astype(BF)


def last_kernel(own, parts):
    return pl.pallas_call(
        last_body,
        out_shape=sds(own.shape, BF),
        in_specs=[VMEM] * 5,
        out_specs=VMEM,
        compiler_params=params(8),
        name="last",
    )(own, *parts)


def join_body(first, own, c0, f1, f2, f3, out):
    split = first.shape[0]
    out[:split, :] = first[...]
    out[split:, :] = (own[...].astype(F32) + 0.5 * total_of((c0, f1, f2, f3))).astype(BF)


def join_kernel(first, own, parts):
    return pl.pallas_call(
        join_body,
        out_shape=sds((T, COL), BF),
        in_specs=[VMEM] * 6,
        out_specs=VMEM,
        compiler_params=params(8),
        name="join",
    )(first, own, *parts)


NORM_ROWS = 128


def row_scale(pieces):
    total = None
    for x in pieces:
        for at in range(0, x.shape[1], 128):
            part = x[:, at : at + 128]
            total = part * part if total is None else total + part * part
    return lax.rsqrt(jnp.sum(total, axis=1, keepdims=True) * (1.0 / D) + EPS)


def ffn_body(
    order, pack, gain, m0, m1, m2, m3, n0, n1, n2, n3, send, keep, weights, rows_x, hid, sem
):
    copies = [
        pltpu.make_async_copy(pack.at[j], weights.at[:, pl.ds(j * 128, 128)], sem)
        for j in range(16)
    ]
    for copy in copies:
        copy.start()
    refs = (m0, m1, m2, m3, n0, n1, n2, n3)

    def norm(b, _):
        rows = pl.ds(pl.multiple_of(b * NORM_ROWS, NORM_ROWS), NORM_ROWS)
        scale = row_scale([r[rows, :].astype(F32) for r in refs])
        for i, r in enumerate(refs):
            cols = pl.ds(pl.multiple_of(order[i] * COL, COL), COL)
            rows_x[rows, cols] = (r[rows, :].astype(F32) * scale * gain[:, cols]).astype(BF)
        return 0

    lax.fori_loop(0, rows_x.shape[0] // NORM_ROWS, norm, 0)
    for copy in copies:
        copy.wait()
    over_k = (((1,), (1,)), ((), ()))
    gate = lax.dot_general(
        rows_x[...], weights[0:FF, :], over_k, preferred_element_type=F32
    )
    up = lax.dot_general(
        rows_x[...], weights[FF : 2 * FF, :], over_k, preferred_element_type=F32
    )
    hid[...] = (silu(gate) * up).astype(BF)
    for half, target in ((1, send), (0, keep)):

        def project(k, _, half=half, target=target):
            cols = pl.ds(pl.multiple_of(order[half * 4 + k] * COL, COL), COL)
            target[k] = jnp.dot(
                hid[...], weights[2 * FF :, cols], preferred_element_type=F32
            ).astype(BF)
            return 0

        lax.fori_loop(0, 4, project, 0)


def ffn_kernel(order, pack, gain, mine, theirs):
    count = mine[0].shape[0]
    return pl.pallas_call(
        ffn_body,
        out_shape=(sds((4, count, COL), BF), sds((4, count, COL), BF)),
        in_specs=[SMEM, pl.BlockSpec(memory_space=pltpu.HBM)] + [VMEM] * 9,
        out_specs=(VMEM,) * 2,
        scratch_shapes=[
            pltpu.VMEM((PACK, D), BF),
            pltpu.VMEM((count, D), BF),
            pltpu.VMEM((count, FF), BF),
            pltpu.SemaphoreType.DMA,
        ],
        compiler_params=params(24),
        cost_estimate=pl.CostEstimate(flops=9_000_000_000, transcendentals=0, bytes_accessed=12_000_000),
        name="ffn",
    )(order, pack, gain, *mine, *theirs)


def turn(array, axis, distance):
    count = lax.axis_size(axis)
    return lax.ppermute(array, axis, [(i, (i + distance) % count) for i in range(count)])


def swap(array):
    return lax.ppermute(array, "c", [(0, 1), (1, 0)])


def reduce_chips(parts):
    c0, c1, c2, c3 = parts
    return c0, turn(c2, "x", 2), turn(c1, "x", 1), turn(c3, "x", -1)


def gather_chips(own):
    return own, turn(own, "x", -1), turn(own, "x", 2), turn(own, "x", 1)


def shards(
    arriving, content, gate, linked, raw, spike, taps_c, taps_p, shift, fading, skip,
    cluster_gain, blender, norm_gain, w_gate, w_up, w_down,
):
    x, c = lax.axis_index("x"), lax.axis_index("c")
    y, z = lax.axis_index("y"), lax.axis_index("z")
    pairs = linked.reshape(T, 256)
    tail = tail_kernel(content, pairs)
    tail, w_gate, w_up, w_down = lax.optimization_barrier((tail, w_gate, w_up, w_down))
    halo = lax.ppermute(tail, SP, [(i, i + 1) for i in range(15)])
    pack = jnp.concatenate([w_gate.T, w_up.T, w_down], axis=0)
    pack = lax.all_gather(pack, SP, axis=0, tiled=True).reshape(16, PACK, 128)
    values, maps, cum, tot, step, entering, payload = state_kernel(
        content, pairs, halo, raw.T, spike.T, shift.reshape(HEADS, 1),
        fading.reshape(HEADS, 1), taps_c, taps_p.reshape(4, 256),
    )
    line = [payload] + [turn(payload, "y", d) for d in (1, 2, 3)]
    local, opened = local_kernel(
        values, maps, cum, step, entering, skip.reshape(HEADS, 1), gate, blender
    )
    local = pltpu.with_memory_space_constraint(local, pltpu.VMEM)
    opened = pltpu.with_memory_space_constraint(opened, pltpu.VMEM)
    mine_cols = lax.dynamic_slice(arriving, (0, (2 * x + c) * COL), (T, COL))
    payload_z, prefix, ahead = line_kernel(y.reshape(1), line)
    lines = [payload_z] + [turn(payload_z, "z", d) for d in (1, 2, 3)]
    steps = jnp.arange(4, dtype=jnp.int32)
    chips = (x + steps) % 4
    order = jnp.concatenate([chips * 2 + c, chips * 2 + (1 - c)]).astype(jnp.int32)
    incoming = incoming_kernel(z.reshape(1), lines, prefix, ahead)
    gain = norm_gain.reshape(1, D)
    mix_args = (incoming, local, maps, tot, opened, cluster_gain.reshape(1, CH), blender)
    spans = ((0, FIRST), (FIRST, SECOND))
    owns, lasts = [], []
    sent, kept = [], []
    for start, count in spans:
        send, keep = mix_kernel(start, count, order, *mix_args)
        sent.append(swap(send))
        kept.append(keep)
    for i, (start, count) in enumerate(spans):
        parts = pair_kernel(kept[i], sent[i])
        parts = reduce_chips(parts)
        owns.append(own_kernel(start, parts, mine_cols))
    pack = pltpu.with_memory_space_constraint(pack, pltpu.HBM)
    for i, (start, count) in enumerate(spans):
        mine = gather_chips(owns[i])
        theirs = tuple(swap(piece) for piece in mine)
        send, keep = ffn_kernel(order, pack, gain, mine, theirs)
        got = swap(send)
        parts = pair_kernel(keep, got)
        lasts.append(reduce_chips(parts))
    return join_kernel(last_kernel(owns[0], lasts[0]), owns[1], lasts[1])


def solution(mesh):
    torus = Mesh(mesh.devices.reshape(4, 4, 4, 2), ("z", "y", "x", "c"))
    tp = ("x", "c")
    return jax.shard_map(
        shards,
        mesh=torus,
        in_specs=(
            P(SP, None), P(SP, tp), P(SP, tp), P(SP, tp, None, None), P(SP, tp), P(SP, tp),
            P(None, tp), P(None, tp, None, None), P(tp), P(tp), P(tp), P(tp), P(tp, None),
            P(), P(SP, tp), P(SP, tp), P(tp, SP),
        ),
        out_specs=P(SP, tp),
        check_vma=False,
    )
```

```python
import functools

import jax
import jax.numpy as jnp
from jax import lax
from jax.experimental import pallas as pl
from jax.experimental.pallas import tpu as pltpu
from jax.sharding import Mesh
from jax.sharding import PartitionSpec as P


BF = jnp.bfloat16
F32 = jnp.float32
EPS = 1e-06
T = 1024
BLK = 128
NB = T // BLK
HEADS = 8
CH = 512
ST = 128
PAIR = 128
HALO = 16
LOGROWS = 16
D = 2048
COL = 256
FF = 704
PACK = 2 * FF + FF
FIRST = 512
SECOND = T - FIRST

SP = ("z", "y")

VMEM = pl.BlockSpec(memory_space=pltpu.VMEM)
SMEM = pl.BlockSpec(memory_space=pltpu.SMEM)
ANY = pl.BlockSpec(memory_space=pl.ANY)


def sds(shape, kind):
    return jax.ShapeDtypeStruct(shape, kind)


def params(mib=48):
    return pltpu.CompilerParams(vmem_limit_bytes=mib * 1024 * 1024)


def silu(x):
    return x * jax.nn.sigmoid(x)


def hi_dot(a, b):
    return jnp.dot(a, b, preferred_element_type=F32, precision=lax.Precision.HIGHEST)


def lane_low():
    return lax.broadcasted_iota(jnp.int32, (1, PAIR), 1) < PAIR // 2


def spread(rows, width, pieces):
    parts, rest = [], rows
    for _ in range(pieces):
        part = rest.astype(BF)
        rest = rest - part.astype(F32)
        parts.append(part)
    head = lax.broadcasted_iota(jnp.int32, (HEADS, HEADS * width), 0)
    lane = lax.broadcasted_iota(jnp.int32, (HEADS, HEADS * width), 1)
    ones = ((lane >= head * width) & (lane < (head + 1) * width)).astype(F32).astype(BF)
    return lax.dot_general(
        jnp.concatenate(parts, axis=0), jnp.concatenate([ones] * pieces, axis=0),
        (((0,), (0,)), ((), ())), preferred_element_type=F32,
    )


def block_lanes(b):
    return pl.ds(pl.multiple_of(b * BLK, BLK), BLK)


def conv_rows(ext, taps):
    total = ext[HALO - 3 : HALO - 3 + BLK] * taps[0:1]
    for k in range(1, 4):
        total = total + ext[HALO - 3 + k : HALO - 3 + k + BLK] * taps[k : k + 1]
    return silu(total).astype(BF)


def column(row):
    own = lax.broadcasted_iota(jnp.int32, (HEADS, HEADS), 0) == lax.broadcasted_iota(
        jnp.int32, (HEADS, HEADS), 1
    )
    spread_row = jnp.broadcast_to(row, (HEADS, HEADS))
    return jnp.sum(jnp.where(own, spread_row, 0.0), axis=1, keepdims=True)


def softplus(x):
    return jnp.maximum(x, 0.0) + jnp.log1p(jnp.exp(-jnp.abs(x)))


def decay_body(
    raw, spike, shift, fading, skip, taps_c, taps_p,
    cum_out, tot_out, step_out, factors, ends, total_out, skip_out, taps_c_out, taps_p_out,
):
    row = lax.broadcasted_iota(jnp.int32, (BLK, BLK), 0)
    col = lax.broadcasted_iota(jnp.int32, (BLK, BLK), 1)
    triu = (row <= col).astype(F32)
    step = softplus(raw[...].astype(F32) + column(shift[...]))
    step_out[...] = step
    log = -jnp.exp(column(fading[...])) * step + spike[...]
    cum = hi_dot(
        jnp.concatenate([log[:, b * BLK : (b + 1) * BLK] for b in range(NB)], axis=0), triu
    )
    prior = jnp.zeros((HEADS, 1), F32)
    for b in range(NB):
        lanes = slice(b * BLK, (b + 1) * BLK)
        here = cum[b * HEADS : (b + 1) * HEADS]
        end = here[:, BLK - 1 : BLK]
        cum_out[:, lanes] = here
        tot_out[:, lanes] = here + prior
        factors[b] = step[:, lanes] * jnp.exp(end - here)
        ends[b] = jnp.broadcast_to(jnp.exp(end), (HEADS, BLK))
        prior = prior + end
    total_out[...] = spread(jnp.broadcast_to(prior, (HEADS, BLK)), 64, 3)[0:8]
    skip_out[...] = spread(jnp.broadcast_to(column(skip[...]), (HEADS, BLK)), 64, 3)[0:8]
    taps_c_out[0:4, :] = taps_c[...].astype(F32)
    wide = taps_p[...].astype(F32)
    taps_p_out[0:4, 0:ST] = wide[:, 0, :]
    taps_p_out[0:4, ST : 2 * ST] = wide[:, 1, :]


def decay_kernel(*args):
    return pl.pallas_call(
        decay_body,
        out_shape=(
            sds((HEADS, T), F32),
            sds((HEADS, T), F32),
            sds((HEADS, T), F32),
            sds((NB, HEADS, BLK), F32),
            sds((NB, HEADS, BLK), F32),
            sds((8, CH), F32),
            sds((8, CH), F32),
            sds((8, CH), F32),
            sds((8, 256), F32),
        ),
        grid=(1,),
        in_specs=[whole(a.shape) for a in args],
        out_specs=(VMEM,) * 9,
        compiler_params=params(8),
        name="decay",
    )(*in_hbm(*args))


def state_body(
    content, pairs, halo, factors, ends, total, taps_c, taps_p,
    values, maps, entering, payload,
    ext_c, ext_p, carry,
):
    ext_c[0:HALO] = halo[:, 0:CH]
    ext_p[0:HALO] = halo[:, CH : CH + 256]
    ext_c[HALO : HALO + T] = content[...]
    ext_p[HALO : HALO + T] = pairs[...]
    carry[...] = jnp.zeros((ST, CH), F32)
    tc = taps_c[...]
    tp = taps_p[...]

    def block(b, _):
        at = pl.multiple_of(b * BLK, BLK)
        rows = pl.ds(at, BLK)
        wide = pl.ds(at, BLK + HALO)
        v = conv_rows(ext_c[wide, :].astype(F32), tc)
        m = conv_rows(ext_p[wide, :].astype(F32), tp)
        values[rows, :] = v
        maps[rows, :] = m
        scaled = (v.astype(F32) * spread(factors[b], 64, 2)).astype(BF)
        added = lax.dot_general(
            m[:, 0:ST], scaled, (((0,), (0,)), ((), ())), preferred_element_type=F32
        )
        old = carry[...]
        entering[b] = old.astype(BF)
        carry[...] = old * spread(ends[b], 64, 2) + added
        return 0

    lax.fori_loop(0, NB, block, 0, unroll=4)
    payload[0:ST, :] = carry[...].astype(BF)
    high = total[...].astype(BF)
    low = (total[...] - high.astype(F32)).astype(BF)
    payload[ST : ST + LOGROWS, :] = jnp.concatenate([high, low], axis=0)


def state_kernel(*args):
    return pl.pallas_call(
        state_body,
        out_shape=(
            sds((T, CH), BF),
            sds((T, 256), BF),
            sds((NB, ST, CH), BF),
            sds((ST + LOGROWS, CH), BF),
        ),
        in_specs=[VMEM] * 8,
        out_specs=(VMEM,) * 4,
        scratch_shapes=[
            pltpu.VMEM((T + HALO, CH), BF),
            pltpu.VMEM((T + HALO, 256), BF),
            pltpu.VMEM((ST, CH), F32),
        ],
        compiler_params=params(12),
        name="state",
    )(*args)


def local_body(values, maps, cum_in, step_in, entering, skip, gate, blend, out, gate_out):
    row = lax.broadcasted_iota(jnp.int32, (BLK, BLK), 0)
    col = lax.broadcasted_iota(jnp.int32, (BLK, BLK), 1)
    causal = col <= row
    low = lane_low()
    gain = skip[0:1, :]

    def block(b, _):
        rows = block_lanes(b)
        v = values[rows, :]
        m = maps[rows, :]
        write, read = m[:, 0:ST], m[:, ST : 2 * ST]
        cum = cum_in[:, rows]
        cum_wide = spread(cum, BLK, 3)
        steps = step_in[:, rows]
        meet = lax.dot_general(
            read, write, (((1,), (1,)), ((), ())), preferred_element_type=F32
        )
        parts = []
        for p in range(HEADS // 2):
            weights = []
            for h in (2 * p, 2 * p + 1):
                gap = cum_wide[:, h * BLK : (h + 1) * BLK] - cum[h : h + 1, :]
                decay = jnp.exp(jnp.where(causal, gap, -jnp.inf))
                weights.append((meet * decay * steps[h : h + 1, :]).astype(BF))
            vp = v[:, p * PAIR : (p + 1) * PAIR]
            none = jnp.zeros_like(vp)
            stacked = jnp.concatenate(
                [jnp.where(low, vp, none), jnp.where(low, none, vp)], axis=0
            )
            parts.append(
                jnp.dot(
                    jnp.concatenate(weights, axis=1), stacked, preferred_element_type=F32
                )
            )
        within = jnp.concatenate(parts, axis=1)
        carried = jnp.dot(read, entering[b], preferred_element_type=F32)
        carried = carried * spread(jnp.exp(cum), 64, 2)
        out[rows, :] = within + carried + v.astype(F32) * gain
        gate_out[rows, :] = silu(gate[rows, :].astype(F32))
        return 0

    lax.fori_loop(0, NB, block, 0)


def local_kernel(*args):
    return pl.pallas_call(
        local_body,
        out_shape=(sds((T, CH), F32), sds((T, CH), F32)),
        in_specs=[VMEM] * 8,
        out_specs=(VMEM,) * 2,
        compiler_params=params(12),
        cost_estimate=pl.CostEstimate(flops=6_000_000_000, transcendentals=0, bytes_accessed=6_000_000),
        name="local",
    )(*args)


def tail_body(content, pairs, out):
    out[:, 0:CH] = content[...]
    out[:, CH : CH + 256] = pairs[...]


def tail_kernel(content, pairs):
    last = T // HALO - 1
    return pl.pallas_call(
        tail_body,
        out_shape=sds((HALO, CH + 256), BF),
        grid=(1,),
        in_specs=[
            pl.BlockSpec((HALO, CH), lambda _: (last, 0)),
            pl.BlockSpec((HALO, 256), lambda _: (0, 0)),
        ],
        out_specs=VMEM,
        compiler_params=params(4),
        name="tail",
    )(content, pairs)


def log_row(ref):
    return ref[ST : ST + 1, :].astype(F32) + ref[ST + 8 : ST + 9, :].astype(F32)


def scan_line(place, refs, state, prefix):
    state[...] = jnp.zeros((ST, CH), F32)
    prefix[...] = jnp.zeros((ST, CH), F32)
    count = len(refs)
    logs = [log_row(r) for r in refs]
    whole = jnp.zeros((1, CH), F32)
    ahead = jnp.zeros((1, CH), F32)
    for j in range(count):
        for d in range(count):

            @pl.when(lax.rem(place - j + count, count) == d)
            def _(d=d):
                if d == 0:
                    prefix[...] = state[...]
                state[...] = state[...] * jnp.exp(logs[d]) + refs[d][0:ST, :].astype(F32)

    for d in range(count):
        whole = whole + logs[d]
        ahead = ahead + jnp.where(place >= d, logs[d], 0.0) if d else ahead
    return whole, ahead


def line_body(place, r0, r1, r2, r3, payload, prefix, ahead_out, state):
    whole, ahead = scan_line(place[0], (r0, r1, r2, r3), state, prefix)
    payload[0:ST, :] = state[...].astype(BF)
    high = whole.astype(BF)
    low = (whole - high.astype(F32)).astype(BF)
    payload[ST : ST + 8, :] = jnp.broadcast_to(high, (8, CH))
    payload[ST + 8 : ST + 16, :] = jnp.broadcast_to(low, (8, CH))
    ahead_out[...] = jnp.broadcast_to(ahead, (8, CH))


def line_kernel(place, received):
    return pl.pallas_call(
        line_body,
        out_shape=(
            sds((ST + LOGROWS, CH), BF),
            sds((ST, CH), F32),
            sds((8, CH), F32),
        ),
        in_specs=[SMEM] + [VMEM] * 4,
        out_specs=(VMEM,) * 3,
        scratch_shapes=[pltpu.VMEM((ST, CH), F32)],
        compiler_params=params(8),
        name="line",
    )(place, *received)


def incoming_body(place, q0, q1, q2, q3, prefix, ahead, incoming, state, prefix_z):
    scan_line(place[0], (q0, q1, q2, q3), state, prefix_z)
    incoming[...] = (prefix_z[...] * jnp.exp(ahead[0:1, :]) + prefix[...]).astype(BF)


def incoming_kernel(place, received, prefix, ahead):
    return pl.pallas_call(
        incoming_body,
        out_shape=sds((ST, CH), BF),
        in_specs=[SMEM] + [VMEM] * 6,
        out_specs=VMEM,
        scratch_shapes=[pltpu.VMEM((ST, CH), F32), pltpu.VMEM((ST, CH), F32)],
        compiler_params=params(8),
        name="incoming",
    )(place, *received, prefix, ahead)


def mix_body(
    start, count, order, incoming, local, maps, tot, gate, gain, blend, send, mixed
):
    rescale = gain[...]

    def block(b, _):
        rows = pl.ds(pl.multiple_of(start + b * BLK, BLK), BLK)
        read = maps[rows, ST : 2 * ST]
        arrived = jnp.dot(read, incoming[...], preferred_element_type=F32)
        mixer = local[rows, :] + arrived * spread(jnp.exp(tot[:, rows]), 64, 2)
        gated = mixer * gate[rows, :]
        scale = lax.rsqrt(jnp.mean(gated * gated, axis=1, keepdims=True) + EPS)
        mixed[pl.ds(pl.multiple_of(b * BLK, BLK), BLK), :] = (gated * scale * rescale).astype(BF)
        return 0

    lax.fori_loop(0, count // BLK, block, 0, unroll=2)
    project(order, 4, mixed, blend, 0, send)


def project(order, first, rows, weights, at, target):
    height = rows.shape[1]
    for k in range(4):
        cols = pl.ds(pl.multiple_of(order[first + k] * COL, COL), COL)
        target[k] = jnp.dot(
            rows[...], weights[at : at + height, cols], preferred_element_type=F32
        ).astype(BF)


def cols_body(col, arriving, out):
    out[...] = arriving[...]


def cols_kernel(col, arriving):
    return pl.pallas_call(
        cols_body,
        out_shape=sds((T, COL), BF),
        grid_spec=pltpu.PrefetchScalarGridSpec(
            num_scalar_prefetch=1,
            grid=(1,),
            in_specs=[pl.BlockSpec((T, COL), lambda _, col: (0, col[0]))],
            out_specs=VMEM,
        ),
        compiler_params=params(4),
        name="cols",
    )(col, pltpu.with_memory_space_constraint(arriving, pltpu.HBM))


def keep_body(at, order, rows, weights, target):
    project(order, 0, rows, weights, at, target)


def keep_kernel(order, rows, weights, at):
    return pl.pallas_call(
        functools.partial(keep_body, at),
        out_shape=sds((4, rows.shape[0], COL), BF),
        in_specs=[SMEM, VMEM, VMEM],
        out_specs=VMEM,
        compiler_params=params(8),
        cost_estimate=pl.CostEstimate(flops=1_000_000_000, transcendentals=0, bytes_accessed=6_000_000),
        name="keep",
    )(order, rows, weights)


def mix_kernel(start, count, order, *args):
    return pl.pallas_call(
        functools.partial(mix_body, start, count),
        out_shape=(sds((4, count, COL), BF), sds((count, CH), BF)),
        in_specs=[SMEM] + [VMEM] * 7,
        out_specs=(VMEM,) * 2,
        compiler_params=params(8),
        cost_estimate=pl.CostEstimate(flops=3_000_000_000, transcendentals=0, bytes_accessed=6_000_000),
        name="mix",
    )(order, *args)


def pair_body(keep, got, c0, c1, c2, c3):
    for k, out in enumerate((c0, c1, c2, c3)):
        out[...] = (keep[k].astype(F32) + got[k].astype(F32)).astype(BF)


def pair_kernel(keep, got):
    count = keep.shape[1]
    return pl.pallas_call(
        pair_body,
        out_shape=(sds((count, COL), BF),) * 4,
        in_specs=[VMEM] * 2,
        out_specs=(VMEM,) * 4,
        compiler_params=params(8),
        name="pair",
    )(keep, got)


def total_of(refs):
    total = refs[0][...].astype(F32)
    for r in refs[1:]:
        total = total + r[...].astype(F32)
    return total


def own_body(start, c0, f1, f2, f3, arriving, out):
    count = out.shape[0]
    base = arriving[start : start + count, :].astype(F32)
    out[...] = (base + total_of((c0, f1, f2, f3))).astype(BF)


def own_kernel(start, parts, arriving):
    count = parts[0].shape[0]
    return pl.pallas_call(
        functools.partial(own_body, start),
        out_shape=sds((count, COL), BF),
        in_specs=[VMEM] * 5,
        out_specs=VMEM,
        compiler_params=params(8),
        name="own",
    )(*parts, arriving)


def last_body(own, c0, f1, f2, f3, out):
    out[...] = (own[...].astype(F32) + 0.5 * total_of((c0, f1, f2, f3))).astype(BF)


def last_kernel(own, parts):
    return pl.pallas_call(
        last_body,
        out_shape=sds(own.shape, BF),
        in_specs=[VMEM] * 5,
        out_specs=VMEM,
        compiler_params=params(8),
        name="last",
    )(own, *parts)


def join_body(first, own, c0, f1, f2, f3, out):
    split = first.shape[0]
    out[:split, :] = first[...]
    out[split:, :] = (own[...].astype(F32) + 0.5 * total_of((c0, f1, f2, f3))).astype(BF)


def join_kernel(first, own, parts):
    return pl.pallas_call(
        join_body,
        out_shape=sds((T, COL), BF),
        in_specs=[VMEM] * 6,
        out_specs=VMEM,
        compiler_params=params(8),
        name="join",
    )(first, own, *parts)


NORM_ROWS = 128


def row_scale(pieces):
    total = None
    for x in pieces:
        for at in range(0, x.shape[1], 128):
            part = x[:, at : at + 128]
            total = part * part if total is None else total + part * part
    return lax.rsqrt(jnp.sum(total, axis=1, keepdims=True) * (1.0 / D) + EPS)


def ffn_rows(order, gain, refs, rows_x):
    def norm(b, _):
        rows = pl.ds(pl.multiple_of(b * NORM_ROWS, NORM_ROWS), NORM_ROWS)
        scale = row_scale([r[rows, :].astype(F32) for r in refs])
        for i, r in enumerate(refs):
            cols = pl.ds(pl.multiple_of(order[i] * COL, COL), COL)
            rows_x[rows, cols] = (r[rows, :].astype(F32) * scale * gain[:, cols]).astype(BF)
        return 0

    lax.fori_loop(0, rows_x.shape[0] // NORM_ROWS, norm, 0)


def ffn_hidden(weights, rows_x, hid):
    over_k = (((1,), (1,)), ((), ()))
    gate = lax.dot_general(
        rows_x[...], weights[0:FF, :], over_k, preferred_element_type=F32
    )
    up = lax.dot_general(
        rows_x[...], weights[FF : 2 * FF, :], over_k, preferred_element_type=F32
    )
    hid[...] = (silu(gate) * up).astype(BF)


def ffn_first_body(
    order, pack, gain, m0, m1, m2, m3, n0, n1, n2, n3, send, hid, weights, rows_x, sems
):
    def copies(part, at, size):
        return [
            pltpu.make_async_copy(
                pack.at[j, pl.ds(at, size), :],
                weights.at[pl.ds(at, size), pl.ds(j * 128, 128)],
                sems.at[part],
            )
            for j in range(16)
        ]

    up, down = copies(0, 0, 2 * FF), copies(1, 2 * FF, FF)
    for copy in up + down:
        copy.start()
    ffn_rows(order, gain, (m0, m1, m2, m3, n0, n1, n2, n3), rows_x)
    for copy in up:
        copy.wait()
    ffn_hidden(weights, rows_x, hid)
    for copy in down:
        copy.wait()
    project(order, 4, hid, weights, 2 * FF, send)


def ffn_next_body(
    order, weights, gain, m0, m1, m2, m3, n0, n1, n2, n3, send, hid, rows_x
):
    ffn_rows(order, gain, (m0, m1, m2, m3, n0, n1, n2, n3), rows_x)
    ffn_hidden(weights, rows_x, hid)
    project(order, 4, hid, weights, 2 * FF, send)


def ffn_kernel(order, weights, gain, pieces, first):
    count = pieces[0].shape[0]
    shapes = (sds((4, count, COL), BF), sds((count, FF), BF))
    scratch = [pltpu.VMEM((count, D), BF)]
    if first:
        shapes += (sds((PACK, D), BF),)
        scratch.append(pltpu.SemaphoreType.DMA((2,)))
        (weights,) = in_hbm(weights)
    return pl.pallas_call(
        ffn_first_body if first else ffn_next_body,
        out_shape=shapes,
        in_specs=[SMEM, HBM if first else VMEM] + [VMEM] * (len(pieces) + 1),
        out_specs=(VMEM,) * len(shapes),
        scratch_shapes=scratch,
        compiler_params=params(14),
        cost_estimate=pl.CostEstimate(flops=9_000_000_000, transcendentals=0, bytes_accessed=12_000_000),
        name="ffn",
    )(order, weights, gain, *pieces)


HBM = pl.BlockSpec(memory_space=pltpu.HBM)


def pack_body(gate, up, down, out, sem):
    copies = [
        pltpu.make_async_copy(part, out.at[pl.ds(i * FF, FF), :], sem)
        for i, part in enumerate((gate, up, down))
    ]
    for copy in copies:
        copy.start()
    for copy in copies:
        copy.wait()


def whole(shape):
    return pl.BlockSpec(shape, lambda _: (0,) * len(shape))


def in_hbm(*arrays):
    return tuple(pltpu.with_memory_space_constraint(a, pltpu.HBM) for a in arrays)


def pack_kernel(*parts):
    return pl.pallas_call(
        pack_body,
        out_shape=sds((PACK, 128), BF),
        in_specs=[HBM] * 3,
        out_specs=VMEM,
        scratch_shapes=[pltpu.SemaphoreType.DMA],
        compiler_params=params(4),
        name="pack",
    )(*in_hbm(*parts))


def turn(array, axis, distance):
    count = lax.axis_size(axis)
    return lax.ppermute(array, axis, [(i, (i + distance) % count) for i in range(count)])


def swap(array):
    return lax.ppermute(array, "c", [(0, 1), (1, 0)])


def reduce_chips(parts):
    c0, c1, c2, c3 = parts
    return c0, turn(c2, "x", 2), turn(c1, "x", 1), turn(c3, "x", -1)


def gather_chips(own):
    return own, turn(own, "x", -1), turn(own, "x", 2), turn(own, "x", 1)


def shards(
    arriving, content, gate, linked, raw, spike, taps_c, taps_p, shift, fading, skip,
    cluster_gain, blender, norm_gain, w_gate, w_up, w_down,
):
    x, c = lax.axis_index("x"), lax.axis_index("c")
    y, z = lax.axis_index("y"), lax.axis_index("z")
    chips = (x + jnp.arange(4, dtype=jnp.int32)) % 4
    order = jnp.concatenate([chips * 2 + c, chips * 2 + (1 - c)]).astype(jnp.int32)
    first_col = (2 * x + c).reshape(1)
    y, z = y.reshape(1), z.reshape(1)
    pack = pack_kernel(w_gate.T, w_up.T, w_down)
    gathered = lax.all_gather(pack, SP, axis=0, tiled=True).reshape(16, PACK, 128)
    linked_tail = linked[T - HALO :].reshape(HALO, 256)
    content_tail, linked_tail, pack = lax.optimization_barrier((content, linked_tail, pack))
    tail = tail_kernel(pltpu.with_memory_space_constraint(content_tail, pltpu.HBM), linked_tail)
    tail, order, first_col, y, z, linked = lax.optimization_barrier(
        (tail, order, first_col, y, z, linked)
    )
    pairs = linked.reshape(T, 256)
    halo = lax.ppermute(tail, SP, [(i, i + 1) for i in range(15)])
    cum, tot, step, factors, ends, total, skip, taps_c, taps_p = decay_kernel(
        raw.T, spike.T, shift.reshape(1, HEADS), fading.reshape(1, HEADS),
        skip.reshape(1, HEADS), taps_c, taps_p.reshape(4, 2, ST),
    )
    values, maps, entering, payload = state_kernel(
        content, pairs, halo, factors, ends, total, taps_c, taps_p
    )
    line = [payload] + [turn(payload, "y", d) for d in (1, 2, 3)]
    local, opened = local_kernel(
        values, maps, cum, step, entering, skip, gate, blender
    )
    mine_cols = cols_kernel(first_col, arriving)
    payload_z, prefix, ahead = line_kernel(y, line)
    lines = [payload_z] + [turn(payload_z, "z", d) for d in (1, 2, 3)]
    incoming = incoming_kernel(z, lines, prefix, ahead)
    gain = norm_gain.reshape(1, D)
    mix_args = (incoming, local, maps, tot, opened, cluster_gain.reshape(1, CH), blender)
    (at_a, rows_a), (at_b, rows_b) = (0, FIRST), (FIRST, SECOND)
    send_a, mixed_a = mix_kernel(at_a, rows_a, order, *mix_args)
    got_a = swap(send_a)
    keep_a = keep_kernel(order, mixed_a, blender, 0)
    parts = pair_kernel(keep_a, got_a)
    parts = reduce_chips(parts)
    own_a = own_kernel(at_a, parts, mine_cols)
    mine_a = gather_chips(own_a)
    send_b, mixed_b = mix_kernel(at_b, rows_b, order, *mix_args)
    got_b = swap(send_b)
    keep_b = keep_kernel(order, mixed_b, blender, 0)
    parts = pair_kernel(keep_b, got_b)
    parts = reduce_chips(parts)
    own_b = own_kernel(at_b, parts, mine_cols)
    mine_b = gather_chips(own_b)
    theirs_a = tuple(swap(piece) for piece in mine_a)
    send, hid, weights = ffn_kernel(order, gathered, gain, (*mine_a, *theirs_a), True)
    got = swap(send)
    keep = keep_kernel(order, hid, weights, 2 * FF)
    parts = pair_kernel(keep, got)
    last_a = reduce_chips(parts)
    theirs_b = tuple(swap(piece) for piece in mine_b)
    send, hid = ffn_kernel(order, weights, gain, (*mine_b, *theirs_b), False)
    got = swap(send)
    keep = keep_kernel(order, hid, weights, 2 * FF)
    parts = pair_kernel(keep, got)
    last_b = reduce_chips(parts)
    return join_kernel(last_kernel(own_a, last_a), own_b, last_b)


def solution(mesh):
    torus = Mesh(mesh.devices.reshape(4, 4, 4, 2), ("z", "y", "x", "c"))
    tp = ("x", "c")
    return jax.shard_map(
        shards,
        mesh=torus,
        in_specs=(
            P(SP, None), P(SP, tp), P(SP, tp), P(SP, tp, None, None), P(SP, tp), P(SP, tp),
            P(None, tp), P(None, tp, None, None), P(tp), P(tp), P(tp), P(tp), P(tp, None),
            P(), P(SP, tp), P(SP, tp), P(tp, SP),
        ),
        out_specs=P(SP, tp),
        check_vma=False,
    )
```

```python
import functools

import jax
import jax.numpy as jnp
from jax import lax
from jax.experimental import pallas as pl
from jax.experimental.pallas import tpu as pltpu
from jax.sharding import Mesh
from jax.sharding import PartitionSpec as P


BF = jnp.bfloat16
F32 = jnp.float32
EPS = 1e-06
T = 1024
BLK = 128
NB = T // BLK
HEADS = 8
CH = 512
ST = 128
PAIR = 128
HALO = 16
LOGROWS = 16
D = 2048
COL = 256
FF = 704
PACK = 2 * FF + FF
FIRST = 512
SECOND = T - FIRST

SP = ("z", "y")

VMEM = pl.BlockSpec(memory_space=pltpu.VMEM)
SMEM = pl.BlockSpec(memory_space=pltpu.SMEM)
HBM = pl.BlockSpec(memory_space=pltpu.HBM)


def sds(shape, kind):
    return jax.ShapeDtypeStruct(shape, kind)


def params(mib=48):
    return pltpu.CompilerParams(vmem_limit_bytes=mib * 1024 * 1024)


def silu(x):
    return x * jax.nn.sigmoid(x)


def hi_dot(a, b):
    return jnp.dot(a, b, preferred_element_type=F32, precision=lax.Precision.HIGHEST)


def lane_low():
    return lax.broadcasted_iota(jnp.int32, (1, PAIR), 1) < PAIR // 2


def spread(rows, width, pieces):
    parts, rest = [], rows
    for _ in range(pieces):
        part = rest.astype(BF)
        rest = rest - part.astype(F32)
        parts.append(part)
    head = lax.broadcasted_iota(jnp.int32, (HEADS, HEADS * width), 0)
    lane = lax.broadcasted_iota(jnp.int32, (HEADS, HEADS * width), 1)
    ones = ((lane >= head * width) & (lane < (head + 1) * width)).astype(F32).astype(BF)
    return lax.dot_general(
        jnp.concatenate(parts, axis=0), jnp.concatenate([ones] * pieces, axis=0),
        (((0,), (0,)), ((), ())), preferred_element_type=F32,
    )


def block_lanes(b):
    return pl.ds(pl.multiple_of(b * BLK, BLK), BLK)


def conv_rows(ext, taps):
    total = ext[HALO - 3 : HALO - 3 + BLK] * taps[0:1]
    for k in range(1, 4):
        total = total + ext[HALO - 3 + k : HALO - 3 + k + BLK] * taps[k : k + 1]
    return silu(total).astype(BF)


def column(row):
    own = lax.broadcasted_iota(jnp.int32, (HEADS, HEADS), 0) == lax.broadcasted_iota(
        jnp.int32, (HEADS, HEADS), 1
    )
    spread_row = jnp.broadcast_to(row, (HEADS, HEADS))
    return jnp.sum(jnp.where(own, spread_row, 0.0), axis=1, keepdims=True)


def in_hbm(*arrays):
    return tuple(pltpu.with_memory_space_constraint(a, pltpu.HBM) for a in arrays)


def softplus(x):
    return jnp.maximum(x, 0.0) + jnp.log1p(jnp.exp(-jnp.abs(x)))


def head_body(
    gate, up, down, raw_in, spike_in, shift_in, fading_in, skip_in, taps_c_in, taps_p_in,
    content_in, pairs_in,
    pack, tail, cum_out, tot_out, step_out, factors, ends, total_out, skip_out, taps_c_out,
    taps_p_out,
    packed, raw, spike, shift, fading, skip, taps_c, taps_p, content, pairs, sems,
):
    weights = [
        pltpu.make_async_copy(part, packed.at[pl.ds(i * FF, FF), :], sems.at[0])
        for i, part in enumerate((gate, up, down))
    ]
    small = [
        pltpu.make_async_copy(source, target, sems.at[1])
        for source, target in (
            (raw_in, raw), (spike_in, spike), (shift_in, shift), (fading_in, fading),
            (skip_in, skip), (taps_c_in, taps_c), (taps_p_in, taps_p),
            (content_in.at[pl.ds(T - HALO, HALO), :], content),
            (pairs_in.at[pl.ds(T - HALO, HALO)], pairs),
        )
    ]
    for copy in weights + small:
        copy.start()
    for copy in weights:
        copy.wait()
    out = pltpu.make_async_copy(packed, pack, sems.at[2])
    out.start()
    for copy in small:
        copy.wait()
    tail[:, 0:CH] = content[...]
    rows = pairs[...].astype(F32)
    tail[:, CH : CH + ST] = rows[:, 0, :].astype(BF)
    tail[:, CH + ST : CH + 2 * ST] = rows[:, 1, :].astype(BF)
    row = lax.broadcasted_iota(jnp.int32, (BLK, BLK), 0)
    col = lax.broadcasted_iota(jnp.int32, (BLK, BLK), 1)
    triu = (row <= col).astype(F32)
    step = softplus(raw[...].astype(F32) + column(shift[...]))
    step_out[...] = step
    log = -jnp.exp(column(fading[...])) * step + spike[...]
    cum = hi_dot(
        jnp.concatenate([log[:, b * BLK : (b + 1) * BLK] for b in range(NB)], axis=0), triu
    )
    prior = jnp.zeros((HEADS, 1), F32)
    for b in range(NB):
        lanes = slice(b * BLK, (b + 1) * BLK)
        here = cum[b * HEADS : (b + 1) * HEADS]
        end = here[:, BLK - 1 : BLK]
        cum_out[:, lanes] = here
        tot_out[:, lanes] = here + prior
        factors[b] = step[:, lanes] * jnp.exp(end - here)
        ends[b] = jnp.broadcast_to(jnp.exp(end), (HEADS, BLK))
        prior = prior + end
    total_out[...] = spread(jnp.broadcast_to(prior, (HEADS, BLK)), 64, 3)[0:8]
    skip_out[...] = spread(jnp.broadcast_to(column(skip[...]), (HEADS, BLK)), 64, 3)[0:8]
    taps_c_out[0:4, :] = taps_c[...].astype(F32)
    wide = taps_p[...].astype(F32)
    taps_p_out[0:4, 0:ST] = wide[:, 0, :]
    taps_p_out[0:4, ST : 2 * ST] = wide[:, 1, :]
    out.wait()


def head_kernel(*args):
    small = args[3:10]
    return pl.pallas_call(
        head_body,
        out_shape=(
            sds((PACK, 128), BF),
            sds((HALO, CH + 256), BF),
            sds((HEADS, T), F32),
            sds((HEADS, T), F32),
            sds((HEADS, T), F32),
            sds((NB, HEADS, BLK), F32),
            sds((NB, HEADS, BLK), F32),
            sds((8, CH), F32),
            sds((8, CH), F32),
            sds((8, CH), F32),
            sds((8, 256), F32),
        ),
        in_specs=[HBM] * len(args),
        out_specs=(HBM,) + (VMEM,) * 10,
        scratch_shapes=[pltpu.VMEM((PACK, 128), BF)]
        + [pltpu.VMEM(a.shape, a.dtype) for a in small]
        + [
            pltpu.VMEM((HALO, CH), BF),
            pltpu.VMEM((HALO, 2, ST), BF),
            pltpu.SemaphoreType.DMA((3,)),
        ],
        compiler_params=params(8),
        name="head",
    )(*in_hbm(*args))


def state_body(
    content, pairs, halo, factors, ends, total, taps_c, taps_p,
    values, maps, entering, payload,
    ext_c, ext_p, carry,
):
    ext_c[0:HALO] = halo[:, 0:CH]
    ext_p[0:HALO] = halo[:, CH : CH + 256]
    ext_c[HALO : HALO + T] = content[...]
    ext_p[HALO : HALO + T] = pairs[...]
    carry[...] = jnp.zeros((ST, CH), F32)
    tc = taps_c[...]
    tp = taps_p[...]

    def block(b, _):
        at = pl.multiple_of(b * BLK, BLK)
        rows = pl.ds(at, BLK)
        wide = pl.ds(at, BLK + HALO)
        v = conv_rows(ext_c[wide, :].astype(F32), tc)
        m = conv_rows(ext_p[wide, :].astype(F32), tp)
        values[rows, :] = v
        maps[rows, :] = m
        scaled = (v.astype(F32) * spread(factors[b], 64, 2)).astype(BF)
        added = lax.dot_general(
            m[:, 0:ST], scaled, (((0,), (0,)), ((), ())), preferred_element_type=F32
        )
        old = carry[...]
        entering[b] = old.astype(BF)
        carry[...] = old * spread(ends[b], 64, 2) + added
        return 0

    lax.fori_loop(0, NB, block, 0, unroll=4)
    payload[0:ST, :] = carry[...].astype(BF)
    high = total[...].astype(BF)
    low = (total[...] - high.astype(F32)).astype(BF)
    payload[ST : ST + LOGROWS, :] = jnp.concatenate([high, low], axis=0)


def state_kernel(*args):
    return pl.pallas_call(
        state_body,
        out_shape=(
            sds((T, CH), BF),
            sds((T, 256), BF),
            sds((NB, ST, CH), BF),
            sds((ST + LOGROWS, CH), BF),
        ),
        in_specs=[VMEM] * 8,
        out_specs=(VMEM,) * 4,
        scratch_shapes=[
            pltpu.VMEM((T + HALO, CH), BF),
            pltpu.VMEM((T + HALO, 256), BF),
            pltpu.VMEM((ST, CH), F32),
        ],
        compiler_params=params(12),
        name="state",
    )(*args)


def local_body(values, maps, cum_in, step_in, entering, skip, gate, blend, out, gate_out):
    row = lax.broadcasted_iota(jnp.int32, (BLK, BLK), 0)
    col = lax.broadcasted_iota(jnp.int32, (BLK, BLK), 1)
    causal = col <= row
    low = lane_low()
    gain = skip[0:1, :]

    def block(b, _):
        rows = block_lanes(b)
        v = values[rows, :]
        m = maps[rows, :]
        write, read = m[:, 0:ST], m[:, ST : 2 * ST]
        cum = cum_in[:, rows]
        cum_wide = spread(cum, BLK, 3)
        steps = step_in[:, rows]
        meet = lax.dot_general(
            read, write, (((1,), (1,)), ((), ())), preferred_element_type=F32
        )
        parts = []
        for p in range(HEADS // 2):
            weights = []
            for h in (2 * p, 2 * p + 1):
                gap = cum_wide[:, h * BLK : (h + 1) * BLK] - cum[h : h + 1, :]
                decay = jnp.exp(jnp.where(causal, gap, -jnp.inf))
                weights.append((meet * decay * steps[h : h + 1, :]).astype(BF))
            vp = v[:, p * PAIR : (p + 1) * PAIR]
            none = jnp.zeros_like(vp)
            stacked = jnp.concatenate(
                [jnp.where(low, vp, none), jnp.where(low, none, vp)], axis=0
            )
            parts.append(
                jnp.dot(
                    jnp.concatenate(weights, axis=1), stacked, preferred_element_type=F32
                )
            )
        within = jnp.concatenate(parts, axis=1)
        carried = jnp.dot(read, entering[b], preferred_element_type=F32)
        carried = carried * spread(jnp.exp(cum), 64, 2)
        out[rows, :] = within + carried + v.astype(F32) * gain
        gate_out[rows, :] = silu(gate[rows, :].astype(F32))
        return 0

    lax.fori_loop(0, NB, block, 0)


def local_kernel(*args):
    return pl.pallas_call(
        local_body,
        out_shape=(sds((T, CH), F32), sds((T, CH), F32)),
        in_specs=[VMEM] * 8,
        out_specs=(VMEM,) * 2,
        compiler_params=params(12),
        cost_estimate=pl.CostEstimate(flops=6_000_000_000, transcendentals=0, bytes_accessed=6_000_000),
        name="local",
    )(*args)


def log_row(ref):
    return ref[ST : ST + 1, :].astype(F32) + ref[ST + 8 : ST + 9, :].astype(F32)


def scan_line(place, refs, state, prefix):
    state[...] = jnp.zeros((ST, CH), F32)
    prefix[...] = jnp.zeros((ST, CH), F32)
    count = len(refs)
    logs = [log_row(r) for r in refs]
    whole = jnp.zeros((1, CH), F32)
    ahead = jnp.zeros((1, CH), F32)
    for j in range(count):
        for d in range(count):

            @pl.when(lax.rem(place - j + count, count) == d)
            def _(d=d):
                if d == 0:
                    prefix[...] = state[...]
                state[...] = state[...] * jnp.exp(logs[d]) + refs[d][0:ST, :].astype(F32)

    for d in range(count):
        whole = whole + logs[d]
        ahead = ahead + jnp.where(place >= d, logs[d], 0.0) if d else ahead
    return whole, ahead


def line_body(place, r0, r1, r2, r3, payload, prefix, ahead_out, state):
    whole, ahead = scan_line(place[0], (r0, r1, r2, r3), state, prefix)
    payload[0:ST, :] = state[...].astype(BF)
    high = whole.astype(BF)
    low = (whole - high.astype(F32)).astype(BF)
    payload[ST : ST + 8, :] = jnp.broadcast_to(high, (8, CH))
    payload[ST + 8 : ST + 16, :] = jnp.broadcast_to(low, (8, CH))
    ahead_out[...] = jnp.broadcast_to(ahead, (8, CH))


def line_kernel(place, received):
    return pl.pallas_call(
        line_body,
        out_shape=(
            sds((ST + LOGROWS, CH), BF),
            sds((ST, CH), F32),
            sds((8, CH), F32),
        ),
        in_specs=[SMEM] + [VMEM] * 4,
        out_specs=(VMEM,) * 3,
        scratch_shapes=[pltpu.VMEM((ST, CH), F32)],
        compiler_params=params(8),
        name="line",
    )(place, *received)


def incoming_body(place, q0, q1, q2, q3, prefix, ahead, incoming, state, prefix_z):
    scan_line(place[0], (q0, q1, q2, q3), state, prefix_z)
    incoming[...] = (prefix_z[...] * jnp.exp(ahead[0:1, :]) + prefix[...]).astype(BF)


def incoming_kernel(place, received, prefix, ahead):
    return pl.pallas_call(
        incoming_body,
        out_shape=sds((ST, CH), BF),
        in_specs=[SMEM] + [VMEM] * 6,
        out_specs=VMEM,
        scratch_shapes=[pltpu.VMEM((ST, CH), F32), pltpu.VMEM((ST, CH), F32)],
        compiler_params=params(8),
        name="incoming",
    )(place, *received, prefix, ahead)


def mix_body(
    start, count, order, incoming, local, maps, tot, gate, gain, blend, send, mixed
):
    rescale = gain[...]

    def block(b, _):
        rows = pl.ds(pl.multiple_of(start + b * BLK, BLK), BLK)
        read = maps[rows, ST : 2 * ST]
        arrived = jnp.dot(read, incoming[...], preferred_element_type=F32)
        mixer = local[rows, :] + arrived * spread(jnp.exp(tot[:, rows]), 64, 2)
        gated = mixer * gate[rows, :]
        scale = lax.rsqrt(jnp.mean(gated * gated, axis=1, keepdims=True) + EPS)
        mixed[pl.ds(pl.multiple_of(b * BLK, BLK), BLK), :] = (gated * scale * rescale).astype(BF)
        return 0

    lax.fori_loop(0, count // BLK, block, 0, unroll=2)
    project(order, 4, mixed, blend, send)


def project(order, first, rows, weights, target):
    for k in range(4):
        cols = pl.ds(pl.multiple_of(order[first + k] * COL, COL), COL)
        target[k] = jnp.dot(
            rows[...], weights[:, cols], preferred_element_type=F32
        ).astype(BF)


def cols_body(col, arriving, out):
    out[...] = arriving[...]


def cols_kernel(col, arriving):
    return pl.pallas_call(
        cols_body,
        out_shape=sds((T, COL), BF),
        grid_spec=pltpu.PrefetchScalarGridSpec(
            num_scalar_prefetch=1,
            grid=(1,),
            in_specs=[pl.BlockSpec((T, COL), lambda _, col: (0, col[0]))],
            out_specs=VMEM,
        ),
        compiler_params=params(4),
        name="cols",
    )(col, *in_hbm(arriving))


def keep_body(order, rows, weights, target):
    project(order, 0, rows, weights, target)


def keep_kernel(order, rows, weights):
    return pl.pallas_call(
        keep_body,
        out_shape=sds((4, rows.shape[0], COL), BF),
        in_specs=[SMEM, VMEM, VMEM],
        out_specs=VMEM,
        compiler_params=params(8),
        cost_estimate=pl.CostEstimate(flops=1_000_000_000, transcendentals=0, bytes_accessed=6_000_000),
        name="keep",
    )(order, rows, weights)


def mix_kernel(start, count, order, *args):
    return pl.pallas_call(
        functools.partial(mix_body, start, count),
        out_shape=(sds((4, count, COL), BF), sds((count, CH), BF)),
        in_specs=[SMEM] + [VMEM] * 7,
        out_specs=(VMEM,) * 2,
        compiler_params=params(8),
        cost_estimate=pl.CostEstimate(flops=3_000_000_000, transcendentals=0, bytes_accessed=6_000_000),
        name="mix",
    )(order, *args)


def pair_body(keep, got, c0, c1, c2, c3):
    for k, out in enumerate((c0, c1, c2, c3)):
        out[...] = (keep[k].astype(F32) + got[k].astype(F32)).astype(BF)


def pair_kernel(keep, got):
    count = keep.shape[1]
    return pl.pallas_call(
        pair_body,
        out_shape=(sds((count, COL), BF),) * 4,
        in_specs=[VMEM] * 2,
        out_specs=(VMEM,) * 4,
        compiler_params=params(8),
        name="pair",
    )(keep, got)


def total_of(refs):
    total = refs[0][...].astype(F32)
    for r in refs[1:]:
        total = total + r[...].astype(F32)
    return total


def own_body(start, c0, f1, f2, f3, arriving, out):
    count = out.shape[0]
    base = arriving[start : start + count, :].astype(F32)
    out[...] = (base + total_of((c0, f1, f2, f3))).astype(BF)


def own_kernel(start, parts, arriving):
    count = parts[0].shape[0]
    return pl.pallas_call(
        functools.partial(own_body, start),
        out_shape=sds((count, COL), BF),
        in_specs=[VMEM] * 5,
        out_specs=VMEM,
        compiler_params=params(8),
        name="own",
    )(*parts, arriving)


def last_body(own, c0, f1, f2, f3, out):
    out[...] = (own[...].astype(F32) + 0.5 * total_of((c0, f1, f2, f3))).astype(BF)


def last_kernel(own, parts):
    return pl.pallas_call(
        last_body,
        out_shape=sds(own.shape, BF),
        in_specs=[VMEM] * 5,
        out_specs=VMEM,
        compiler_params=params(8),
        name="last",
    )(own, *parts)


def join_body(first, own, c0, f1, f2, f3, out):
    split = first.shape[0]
    out[:split, :] = first[...]
    out[split:, :] = (own[...].astype(F32) + 0.5 * total_of((c0, f1, f2, f3))).astype(BF)


def join_kernel(first, own, parts):
    return pl.pallas_call(
        join_body,
        out_shape=sds((T, COL), BF),
        in_specs=[VMEM] * 6,
        out_specs=VMEM,
        compiler_params=params(8),
        name="join",
    )(first, own, *parts)


NORM_ROWS = 128


def row_scale(pieces):
    total = None
    for x in pieces:
        for at in range(0, x.shape[1], 128):
            part = x[:, at : at + 128]
            total = part * part if total is None else total + part * part
    return lax.rsqrt(jnp.sum(total, axis=1, keepdims=True) * (1.0 / D) + EPS)


def ffn_rows(order, gain, refs, rows_x):
    def norm(b, _):
        rows = pl.ds(pl.multiple_of(b * NORM_ROWS, NORM_ROWS), NORM_ROWS)
        scale = row_scale([r[rows, :].astype(F32) for r in refs])
        for i, r in enumerate(refs):
            cols = pl.ds(pl.multiple_of(order[i] * COL, COL), COL)
            rows_x[rows, cols] = (r[rows, :].astype(F32) * scale * gain[:, cols]).astype(BF)
        return 0

    lax.fori_loop(0, rows_x.shape[0] // NORM_ROWS, norm, 0)


def ffn_hidden(weights, rows_x, hid, at, width):
    over_k = (((1,), (1,)), ((), ()))

    def columns(at):
        return jnp.concatenate([weights[j, at : at + width, :] for j in range(16)], axis=1)

    gate = lax.dot_general(rows_x[...], columns(at), over_k, preferred_element_type=F32)
    up = lax.dot_general(rows_x[...], columns(FF + at), over_k, preferred_element_type=F32)
    hid[:, at : at + width] = (silu(gate) * up).astype(BF)


def project_down(order, first, hid, weights, target):
    for k in range(4):
        spot = 2 * order[first + k]
        both = jnp.concatenate(
            [weights[spot, 2 * FF :, :], weights[spot + 1, 2 * FF :, :]], axis=1
        )
        target[k] = jnp.dot(hid[...], both, preferred_element_type=F32).astype(BF)


def ffn_first_body(
    order, pack, gain, m0, m1, m2, m3, n0, n1, n2, n3, send, hid, weights, rows_x, sems
):
    def copies(sem, *spans):
        return [
            pltpu.make_async_copy(
                pack.at[:, pl.ds(at, size), :], weights.at[:, pl.ds(at, size), :], sems.at[sem]
            )
            for at, size in spans
        ]

    halves = ((0, 512), (512, FF - 512))
    parts = [
        copies(i, (at, width), (FF + at, width)) for i, (at, width) in enumerate(halves)
    ]
    parts.append(copies(2, (2 * FF, FF)))
    for part in parts:
        for copy in part:
            copy.start()
    ffn_rows(order, gain, (m0, m1, m2, m3, n0, n1, n2, n3), rows_x)
    for part, (at, width) in zip(parts, halves):
        for copy in part:
            copy.wait()
        ffn_hidden(weights, rows_x, hid, at, width)
    for copy in parts[2]:
        copy.wait()
    project_down(order, 4, hid, weights, send)


def ffn_next_body(
    order, weights, gain, m0, m1, m2, m3, n0, n1, n2, n3, send, hid, rows_x
):
    ffn_rows(order, gain, (m0, m1, m2, m3, n0, n1, n2, n3), rows_x)
    ffn_hidden(weights, rows_x, hid, 0, FF)
    project_down(order, 4, hid, weights, send)


def ffn_kernel(order, weights, gain, pieces, first):
    count = pieces[0].shape[0]
    shapes = (sds((4, count, COL), BF), sds((count, FF), BF))
    scratch = [pltpu.VMEM((count, D), BF)]
    if first:
        shapes += (sds((16, PACK, 128), BF),)
        scratch.append(pltpu.SemaphoreType.DMA((3,)))
        (weights,) = in_hbm(weights)
    return pl.pallas_call(
        ffn_first_body if first else ffn_next_body,
        out_shape=shapes,
        in_specs=[SMEM, HBM if first else VMEM] + [VMEM] * (len(pieces) + 1),
        out_specs=(VMEM,) * len(shapes),
        scratch_shapes=scratch,
        compiler_params=params(14),
        cost_estimate=pl.CostEstimate(flops=9_000_000_000, transcendentals=0, bytes_accessed=12_000_000),
        name="ffn",
    )(order, weights, gain, *pieces)


def keep_down_body(order, hid, weights, target):
    project_down(order, 0, hid, weights, target)


def keep_down_kernel(order, hid, weights):
    return pl.pallas_call(
        keep_down_body,
        out_shape=sds((4, hid.shape[0], COL), BF),
        in_specs=[SMEM, VMEM, VMEM],
        out_specs=VMEM,
        compiler_params=params(8),
        cost_estimate=pl.CostEstimate(flops=1_000_000_000, transcendentals=0, bytes_accessed=6_000_000),
        name="keep_down",
    )(order, hid, weights)


def turn(array, axis, distance):
    count = lax.axis_size(axis)
    return lax.ppermute(array, axis, [(i, (i + distance) % count) for i in range(count)])


def swap(array):
    return lax.ppermute(array, "c", [(0, 1), (1, 0)])


def reduce_chips(parts):
    c0, c1, c2, c3 = parts
    far = turn(c2, "x", 2)
    return c0, far, turn(c1, "x", 1), turn(c3, "x", -1)


def gather_chips(own):
    far = turn(own, "x", 2)
    return own, turn(own, "x", -1), far, turn(own, "x", 1)


def shards(
    arriving, content, gate, linked, raw, spike, taps_c, taps_p, shift, fading, skip,
    cluster_gain, blender, norm_gain, w_gate, w_up, w_down,
):
    x, c = lax.axis_index("x"), lax.axis_index("c")
    y, z = lax.axis_index("y"), lax.axis_index("z")
    chips = (x + jnp.arange(4, dtype=jnp.int32)) % 4
    order = jnp.concatenate([chips * 2 + c, chips * 2 + (1 - c)]).astype(jnp.int32)
    first_col = (2 * x + c).reshape(1)
    y, z = y.reshape(1), z.reshape(1)
    pack, tail, cum, tot, step, factors, ends, total, skip, taps_c, taps_p = head_kernel(
        w_gate.T, w_up.T, w_down, raw.T, spike.T, shift.reshape(1, HEADS),
        fading.reshape(1, HEADS), skip.reshape(1, HEADS), taps_c, taps_p.reshape(4, 2, ST),
        content, linked.reshape(T, 2, ST),
    )
    pack, tail, order, first_col, y, z, linked = lax.optimization_barrier(
        (pack, tail, order, first_col, y, z, linked)
    )
    gathered = lax.all_gather(pack, SP, axis=0, tiled=True).reshape(16, PACK, 128)
    pairs = linked.reshape(T, 256)
    halo = lax.ppermute(tail, SP, [(i, i + 1) for i in range(15)])
    values, maps, entering, payload = state_kernel(
        content, pairs, halo, factors, ends, total, taps_c, taps_p
    )
    line = [payload] + [turn(payload, "y", d) for d in (1, 2, 3)]
    local, opened = local_kernel(
        values, maps, cum, step, entering, skip, gate, blender
    )
    mine_cols = cols_kernel(first_col, arriving)
    payload_z, prefix, ahead = line_kernel(y, line)
    lines = [payload_z] + [turn(payload_z, "z", d) for d in (1, 2, 3)]
    incoming = incoming_kernel(z, lines, prefix, ahead)
    gain = norm_gain.reshape(1, D)
    mix_args = (incoming, local, maps, tot, opened, cluster_gain.reshape(1, CH), blender)
    (at_a, rows_a), (at_b, rows_b) = (0, FIRST), (FIRST, SECOND)
    send_a, mixed_a = mix_kernel(at_a, rows_a, order, *mix_args)
    got_a = swap(send_a)
    keep_a = keep_kernel(order, mixed_a, blender)
    parts = pair_kernel(keep_a, got_a)
    parts = reduce_chips(parts)
    own_a = own_kernel(at_a, parts, mine_cols)
    mine_a = gather_chips(own_a)
    send_b, mixed_b = mix_kernel(at_b, rows_b, order, *mix_args)
    got_b = swap(send_b)
    keep_b = keep_kernel(order, mixed_b, blender)
    parts = pair_kernel(keep_b, got_b)
    parts = reduce_chips(parts)
    own_b = own_kernel(at_b, parts, mine_cols)
    mine_b = gather_chips(own_b)
    theirs_a = tuple(swap(piece) for piece in mine_a)
    send, hid, weights = ffn_kernel(order, gathered, gain, (*mine_a, *theirs_a), True)
    got = swap(send)
    keep = keep_down_kernel(order, hid, weights)
    parts = pair_kernel(keep, got)
    last_a = reduce_chips(parts)
    theirs_b = tuple(swap(piece) for piece in mine_b)
    send, hid = ffn_kernel(order, weights, gain, (*mine_b, *theirs_b), False)
    got = swap(send)
    keep = keep_down_kernel(order, hid, weights)
    parts = pair_kernel(keep, got)
    last_b = reduce_chips(parts)
    return join_kernel(last_kernel(own_a, last_a), own_b, last_b)


def solution(mesh):
    torus = Mesh(mesh.devices.reshape(4, 4, 4, 2), ("z", "y", "x", "c"))
    tp = ("x", "c")
    return jax.shard_map(
        shards,
        mesh=torus,
        in_specs=(
            P(SP, None), P(SP, tp), P(SP, tp), P(SP, tp, None, None), P(SP, tp), P(SP, tp),
            P(None, tp), P(None, tp, None, None), P(tp), P(tp), P(tp), P(tp), P(tp, None),
            P(), P(SP, tp), P(SP, tp), P(tp, SP),
        ),
        out_specs=P(SP, tp),
        check_vma=False,
    )
```

```python
import functools

import jax
import jax.numpy as jnp
from jax import lax
from jax.experimental import pallas as pl
from jax.experimental.pallas import tpu as pltpu
from jax.sharding import Mesh
from jax.sharding import PartitionSpec as P


BF = jnp.bfloat16
F32 = jnp.float32
EPS = 1e-06
T = 1024
BLK = 128
NB = T // BLK
HEADS = 8
CH = 512
ST = 128
PAIR = 128
HALO = 16
LOGROWS = 16
D = 2048
COL = 256
FF = 704
PACK = 2 * FF + FF
FIRST = 512
SECOND = T - FIRST

SP = ("z", "y")

VMEM = pl.BlockSpec(memory_space=pltpu.VMEM)
SMEM = pl.BlockSpec(memory_space=pltpu.SMEM)
HBM = pl.BlockSpec(memory_space=pltpu.HBM)


def sds(shape, kind):
    return jax.ShapeDtypeStruct(shape, kind)


def params(mib=48):
    return pltpu.CompilerParams(vmem_limit_bytes=mib * 1024 * 1024)


def silu(x):
    return x * jax.nn.sigmoid(x)


def hi_dot(a, b):
    return jnp.dot(a, b, preferred_element_type=F32, precision=lax.Precision.HIGHEST)


def lane_low():
    return lax.broadcasted_iota(jnp.int32, (1, PAIR), 1) < PAIR // 2


def spread(rows, width, pieces):
    parts, rest = [], rows
    for _ in range(pieces):
        part = rest.astype(BF)
        rest = rest - part.astype(F32)
        parts.append(part)
    head = lax.broadcasted_iota(jnp.int32, (HEADS, HEADS * width), 0)
    lane = lax.broadcasted_iota(jnp.int32, (HEADS, HEADS * width), 1)
    ones = ((lane >= head * width) & (lane < (head + 1) * width)).astype(F32).astype(BF)
    return lax.dot_general(
        jnp.concatenate(parts, axis=0), jnp.concatenate([ones] * pieces, axis=0),
        (((0,), (0,)), ((), ())), preferred_element_type=F32,
    )


def block_lanes(b):
    return pl.ds(pl.multiple_of(b * BLK, BLK), BLK)


def conv_rows(ext, taps):
    total = ext[HALO - 3 : HALO - 3 + BLK] * taps[0:1]
    for k in range(1, 4):
        total = total + ext[HALO - 3 + k : HALO - 3 + k + BLK] * taps[k : k + 1]
    return silu(total).astype(BF)


def column(row):
    own = lax.broadcasted_iota(jnp.int32, (HEADS, HEADS), 0) == lax.broadcasted_iota(
        jnp.int32, (HEADS, HEADS), 1
    )
    spread_row = jnp.broadcast_to(row, (HEADS, HEADS))
    return jnp.sum(jnp.where(own, spread_row, 0.0), axis=1, keepdims=True)


def in_hbm(*arrays):
    return tuple(pltpu.with_memory_space_constraint(a, pltpu.HBM) for a in arrays)


def softplus(x):
    return jnp.maximum(x, 0.0) + jnp.log1p(jnp.exp(-jnp.abs(x)))


def head_body(
    gate, up, down, raw_in, spike_in, shift_in, fading_in, skip_in, taps_c_in, taps_p_in,
    content_in, pairs_in,
    pack, tail, cum_out, tot_out, step_out, factors, ends, total_out, skip_out, taps_c_out,
    taps_p_out,
    packed, raw, spike, shift, fading, skip, taps_c, taps_p, content, pairs, sems,
):
    weights = [
        pltpu.make_async_copy(part, packed.at[pl.ds(i * FF, FF), :], sems.at[0])
        for i, part in enumerate((gate, up, down))
    ]
    small = [
        pltpu.make_async_copy(source, target, sems.at[1])
        for source, target in (
            (raw_in, raw), (spike_in, spike), (shift_in, shift), (fading_in, fading),
            (skip_in, skip), (taps_c_in, taps_c), (taps_p_in, taps_p),
            (content_in.at[pl.ds(T - HALO, HALO), :], content),
            (pairs_in.at[pl.ds(T - HALO, HALO)], pairs),
        )
    ]
    for copy in weights + small:
        copy.start()
    for copy in weights:
        copy.wait()
    out = pltpu.make_async_copy(packed, pack, sems.at[2])
    out.start()
    for copy in small:
        copy.wait()
    tail[:, 0:CH] = content[...]
    rows = pairs[...].astype(F32)
    tail[:, CH : CH + ST] = rows[:, 0, :].astype(BF)
    tail[:, CH + ST : CH + 2 * ST] = rows[:, 1, :].astype(BF)
    row = lax.broadcasted_iota(jnp.int32, (BLK, BLK), 0)
    col = lax.broadcasted_iota(jnp.int32, (BLK, BLK), 1)
    triu = (row <= col).astype(F32)
    step = softplus(raw[...].astype(F32) + column(shift[...]))
    step_out[...] = step
    log = -jnp.exp(column(fading[...])) * step + spike[...]
    cum = hi_dot(
        jnp.concatenate([log[:, b * BLK : (b + 1) * BLK] for b in range(NB)], axis=0), triu
    )
    prior = jnp.zeros((HEADS, 1), F32)
    for b in range(NB):
        lanes = slice(b * BLK, (b + 1) * BLK)
        here = cum[b * HEADS : (b + 1) * HEADS]
        end = here[:, BLK - 1 : BLK]
        cum_out[:, lanes] = here
        tot_out[:, lanes] = here + prior
        factors[b] = step[:, lanes] * jnp.exp(end - here)
        ends[b] = jnp.broadcast_to(jnp.exp(end), (HEADS, BLK))
        prior = prior + end
    total_out[...] = spread(jnp.broadcast_to(prior, (HEADS, BLK)), 64, 3)[0:8]
    skip_out[...] = spread(jnp.broadcast_to(column(skip[...]), (HEADS, BLK)), 64, 3)[0:8]
    taps_c_out[0:4, :] = taps_c[...].astype(F32)
    wide = taps_p[...].astype(F32)
    taps_p_out[0:4, 0:ST] = wide[:, 0, :]
    taps_p_out[0:4, ST : 2 * ST] = wide[:, 1, :]
    out.wait()


def head_kernel(*args):
    small = args[3:10]
    return pl.pallas_call(
        head_body,
        out_shape=(
            sds((PACK, 128), BF),
            sds((HALO, CH + 256), BF),
            sds((HEADS, T), F32),
            sds((HEADS, T), F32),
            sds((HEADS, T), F32),
            sds((NB, HEADS, BLK), F32),
            sds((NB, HEADS, BLK), F32),
            sds((8, CH), F32),
            sds((8, CH), F32),
            sds((8, CH), F32),
            sds((8, 256), F32),
        ),
        in_specs=[HBM] * len(args),
        out_specs=(HBM,) + (VMEM,) * 10,
        scratch_shapes=[pltpu.VMEM((PACK, 128), BF)]
        + [pltpu.VMEM(a.shape, a.dtype) for a in small]
        + [
            pltpu.VMEM((HALO, CH), BF),
            pltpu.VMEM((HALO, 2, ST), BF),
            pltpu.SemaphoreType.DMA((3,)),
        ],
        compiler_params=params(8),
        name="head",
    )(*in_hbm(*args))


def state_body(
    content, pairs, halo, factors, ends, total, taps_c, taps_p,
    values, maps, entering, payload,
    ext_c, ext_p, carry,
):
    ext_c[0:HALO] = halo[:, 0:CH]
    ext_p[0:HALO] = halo[:, CH : CH + 256]
    ext_c[HALO : HALO + T] = content[...]
    ext_p[HALO : HALO + T] = pairs[...]
    carry[...] = jnp.zeros((ST, CH), F32)
    tc = taps_c[...]
    tp = taps_p[...]

    def block(b, _):
        at = pl.multiple_of(b * BLK, BLK)
        rows = pl.ds(at, BLK)
        wide = pl.ds(at, BLK + HALO)
        v = conv_rows(ext_c[wide, :].astype(F32), tc)
        m = conv_rows(ext_p[wide, :].astype(F32), tp)
        values[rows, :] = v
        maps[rows, :] = m
        scaled = (v.astype(F32) * spread(factors[b], 64, 2)).astype(BF)
        added = lax.dot_general(
            m[:, 0:ST], scaled, (((0,), (0,)), ((), ())), preferred_element_type=F32
        )
        old = carry[...]
        entering[b] = old.astype(BF)
        carry[...] = old * spread(ends[b], 64, 2) + added
        return 0

    lax.fori_loop(0, NB, block, 0, unroll=8)
    payload[0:ST, :] = carry[...].astype(BF)
    high = total[...].astype(BF)
    low = (total[...] - high.astype(F32)).astype(BF)
    payload[ST : ST + LOGROWS, :] = jnp.concatenate([high, low], axis=0)


def state_kernel(*args):
    return pl.pallas_call(
        state_body,
        out_shape=(
            sds((T, CH), BF),
            sds((T, 256), BF),
            sds((NB, ST, CH), BF),
            sds((ST + LOGROWS, CH), BF),
        ),
        in_specs=[VMEM] * 8,
        out_specs=(VMEM,) * 4,
        scratch_shapes=[
            pltpu.VMEM((T + HALO, CH), BF),
            pltpu.VMEM((T + HALO, 256), BF),
            pltpu.VMEM((ST, CH), F32),
        ],
        compiler_params=params(12),
        name="state",
    )(*args)


def local_body(values, maps, cum_in, step_in, entering, skip, gate, blend, out, gate_out):
    row = lax.broadcasted_iota(jnp.int32, (BLK, BLK), 0)
    col = lax.broadcasted_iota(jnp.int32, (BLK, BLK), 1)
    causal = col <= row
    low = lane_low()
    gain = skip[0:1, :]

    def block(b, _):
        rows = block_lanes(b)
        v = values[rows, :]
        m = maps[rows, :]
        write, read = m[:, 0:ST], m[:, ST : 2 * ST]
        cum = cum_in[:, rows]
        cum_wide = spread(cum, BLK, 3)
        steps = step_in[:, rows]
        meet = lax.dot_general(
            read, write, (((1,), (1,)), ((), ())), preferred_element_type=F32
        )
        parts = []
        for p in range(HEADS // 2):
            weights = []
            for h in (2 * p, 2 * p + 1):
                gap = cum_wide[:, h * BLK : (h + 1) * BLK] - cum[h : h + 1, :]
                decay = jnp.exp(jnp.where(causal, gap, -jnp.inf))
                weights.append((meet * decay * steps[h : h + 1, :]).astype(BF))
            vp = v[:, p * PAIR : (p + 1) * PAIR]
            none = jnp.zeros_like(vp)
            stacked = jnp.concatenate(
                [jnp.where(low, vp, none), jnp.where(low, none, vp)], axis=0
            )
            parts.append(
                jnp.dot(
                    jnp.concatenate(weights, axis=1), stacked, preferred_element_type=F32
                )
            )
        within = jnp.concatenate(parts, axis=1)
        carried = jnp.dot(read, entering[b], preferred_element_type=F32)
        carried = carried * spread(jnp.exp(cum), 64, 2)
        out[rows, :] = within + carried + v.astype(F32) * gain
        gate_out[rows, :] = silu(gate[rows, :].astype(F32))
        return 0

    lax.fori_loop(0, NB, block, 0)


def local_kernel(*args):
    return pl.pallas_call(
        local_body,
        out_shape=(sds((T, CH), F32), sds((T, CH), F32)),
        in_specs=[VMEM] * 8,
        out_specs=(VMEM,) * 2,
        compiler_params=params(12),
        cost_estimate=pl.CostEstimate(flops=6_000_000_000, transcendentals=0, bytes_accessed=6_000_000),
        name="local",
    )(*args)


def log_row(ref):
    return ref[ST : ST + 1, :].astype(F32) + ref[ST + 8 : ST + 9, :].astype(F32)


def scan_line(place, refs, state, prefix):
    state[...] = jnp.zeros((ST, CH), F32)
    prefix[...] = jnp.zeros((ST, CH), F32)
    count = len(refs)
    logs = [log_row(r) for r in refs]
    whole = jnp.zeros((1, CH), F32)
    ahead = jnp.zeros((1, CH), F32)
    for j in range(count):
        for d in range(count):

            @pl.when(lax.rem(place - j + count, count) == d)
            def _(d=d):
                if d == 0:
                    prefix[...] = state[...]
                state[...] = state[...] * jnp.exp(logs[d]) + refs[d][0:ST, :].astype(F32)

    for d in range(count):
        whole = whole + logs[d]
        ahead = ahead + jnp.where(place >= d, logs[d], 0.0) if d else ahead
    return whole, ahead


def line_body(place, r0, r1, r2, r3, payload, prefix, ahead_out, state):
    whole, ahead = scan_line(place[0], (r0, r1, r2, r3), state, prefix)
    payload[0:ST, :] = state[...].astype(BF)
    high = whole.astype(BF)
    low = (whole - high.astype(F32)).astype(BF)
    payload[ST : ST + 8, :] = jnp.broadcast_to(high, (8, CH))
    payload[ST + 8 : ST + 16, :] = jnp.broadcast_to(low, (8, CH))
    ahead_out[...] = jnp.broadcast_to(ahead, (8, CH))


def line_kernel(place, received):
    return pl.pallas_call(
        line_body,
        out_shape=(
            sds((ST + LOGROWS, CH), BF),
            sds((ST, CH), F32),
            sds((8, CH), F32),
        ),
        in_specs=[SMEM] + [VMEM] * 4,
        out_specs=(VMEM,) * 3,
        scratch_shapes=[pltpu.VMEM((ST, CH), F32)],
        compiler_params=params(8),
        name="line",
    )(place, *received)


def incoming_body(place, q0, q1, q2, q3, prefix, ahead, incoming, state, prefix_z):
    scan_line(place[0], (q0, q1, q2, q3), state, prefix_z)
    incoming[...] = (prefix_z[...] * jnp.exp(ahead[0:1, :]) + prefix[...]).astype(BF)


def incoming_kernel(place, received, prefix, ahead):
    return pl.pallas_call(
        incoming_body,
        out_shape=sds((ST, CH), BF),
        in_specs=[SMEM] + [VMEM] * 6,
        out_specs=VMEM,
        scratch_shapes=[pltpu.VMEM((ST, CH), F32), pltpu.VMEM((ST, CH), F32)],
        compiler_params=params(8),
        name="incoming",
    )(place, *received, prefix, ahead)


def mix_body(
    start, count, order, incoming, local, maps, tot, gate, gain, blend, send, mixed
):
    rescale = gain[...]

    def block(b, _):
        rows = pl.ds(pl.multiple_of(start + b * BLK, BLK), BLK)
        read = maps[rows, ST : 2 * ST]
        arrived = jnp.dot(read, incoming[...], preferred_element_type=F32)
        mixer = local[rows, :] + arrived * spread(jnp.exp(tot[:, rows]), 64, 2)
        gated = mixer * gate[rows, :]
        scale = lax.rsqrt(jnp.mean(gated * gated, axis=1, keepdims=True) + EPS)
        mixed[pl.ds(pl.multiple_of(b * BLK, BLK), BLK), :] = (gated * scale * rescale).astype(BF)
        return 0

    lax.fori_loop(0, count // BLK, block, 0, unroll=4)
    project(order, 4, mixed, blend, send)


def project(order, first, rows, weights, target):
    for k in range(4):
        cols = pl.ds(pl.multiple_of(order[first + k] * COL, COL), COL)
        target[k] = jnp.dot(
            rows[...], weights[:, cols], preferred_element_type=F32
        ).astype(BF)


def cols_body(col, arriving, out):
    out[...] = arriving[...]


def cols_kernel(col, arriving):
    return pl.pallas_call(
        cols_body,
        out_shape=sds((T, COL), BF),
        grid_spec=pltpu.PrefetchScalarGridSpec(
            num_scalar_prefetch=1,
            grid=(1,),
            in_specs=[pl.BlockSpec((T, COL), lambda _, col: (0, col[0]))],
            out_specs=VMEM,
        ),
        compiler_params=params(4),
        name="cols",
    )(col, *in_hbm(arriving))


def keep_body(order, rows, weights, target):
    project(order, 0, rows, weights, target)


def keep_kernel(order, rows, weights):
    return pl.pallas_call(
        keep_body,
        out_shape=sds((4, rows.shape[0], COL), BF),
        in_specs=[SMEM, VMEM, VMEM],
        out_specs=VMEM,
        compiler_params=params(8),
        cost_estimate=pl.CostEstimate(flops=1_000_000_000, transcendentals=0, bytes_accessed=6_000_000),
        name="keep",
    )(order, rows, weights)


def mix_kernel(start, count, order, *args):
    return pl.pallas_call(
        functools.partial(mix_body, start, count),
        out_shape=(sds((4, count, COL), BF), sds((count, CH), BF)),
        in_specs=[SMEM] + [VMEM] * 7,
        out_specs=(VMEM,) * 2,
        compiler_params=params(8),
        cost_estimate=pl.CostEstimate(flops=3_000_000_000, transcendentals=0, bytes_accessed=6_000_000),
        name="mix",
    )(order, *args)


def pair_body(keep, got, c0, c1, c2, c3):
    for k, out in enumerate((c0, c1, c2, c3)):
        out[...] = (keep[k].astype(F32) + got[k].astype(F32)).astype(BF)


def pair_kernel(keep, got):
    count = keep.shape[1]
    return pl.pallas_call(
        pair_body,
        out_shape=(sds((count, COL), BF),) * 4,
        in_specs=[VMEM] * 2,
        out_specs=(VMEM,) * 4,
        compiler_params=params(8),
        name="pair",
    )(keep, got)


def total_of(refs):
    total = refs[0][...].astype(F32)
    for r in refs[1:]:
        total = total + r[...].astype(F32)
    return total


def own_body(start, c0, f1, f2, f3, arriving, out):
    count = out.shape[0]
    base = arriving[start : start + count, :].astype(F32)
    out[...] = (base + total_of((c0, f1, f2, f3))).astype(BF)


def own_kernel(start, parts, arriving):
    count = parts[0].shape[0]
    return pl.pallas_call(
        functools.partial(own_body, start),
        out_shape=sds((count, COL), BF),
        in_specs=[VMEM] * 5,
        out_specs=VMEM,
        compiler_params=params(8),
        name="own",
    )(*parts, arriving)


def last_body(own, c0, f1, f2, f3, out):
    out[...] = (own[...].astype(F32) + 0.5 * total_of((c0, f1, f2, f3))).astype(BF)


def last_kernel(own, parts):
    return pl.pallas_call(
        last_body,
        out_shape=sds(own.shape, BF),
        in_specs=[VMEM] * 5,
        out_specs=VMEM,
        compiler_params=params(8),
        name="last",
    )(own, *parts)


def join_body(first, own, c0, f1, f2, f3, out):
    split = first.shape[0]
    out[:split, :] = first[...]
    out[split:, :] = (own[...].astype(F32) + 0.5 * total_of((c0, f1, f2, f3))).astype(BF)


def join_kernel(first, own, parts):
    return pl.pallas_call(
        join_body,
        out_shape=sds((T, COL), BF),
        in_specs=[VMEM] * 6,
        out_specs=VMEM,
        compiler_params=params(8),
        name="join",
    )(first, own, *parts)


NORM_ROWS = 128


def row_scale(pieces):
    total = None
    for x in pieces:
        for at in range(0, x.shape[1], 128):
            part = x[:, at : at + 128]
            total = part * part if total is None else total + part * part
    return lax.rsqrt(jnp.sum(total, axis=1, keepdims=True) * (1.0 / D) + EPS)


def ffn_rows(order, gain, refs, rows_x):
    def norm(b, _):
        rows = pl.ds(pl.multiple_of(b * NORM_ROWS, NORM_ROWS), NORM_ROWS)
        scale = row_scale([r[rows, :].astype(F32) for r in refs])
        for i, r in enumerate(refs):
            cols = pl.ds(pl.multiple_of(order[i] * COL, COL), COL)
            rows_x[rows, cols] = (r[rows, :].astype(F32) * scale * gain[:, cols]).astype(BF)
        return 0

    lax.fori_loop(0, rows_x.shape[0] // NORM_ROWS, norm, 0)


def ffn_hidden(weights, rows_x, hid, at, width):
    over_k = (((1,), (1,)), ((), ()))

    def columns(at):
        return jnp.concatenate([weights[j, at : at + width, :] for j in range(16)], axis=1)

    gate = lax.dot_general(rows_x[...], columns(at), over_k, preferred_element_type=F32)
    up = lax.dot_general(rows_x[...], columns(FF + at), over_k, preferred_element_type=F32)
    hid[:, at : at + width] = (silu(gate) * up).astype(BF)


def project_down(order, first, hid, weights, target):
    for k in range(4):
        spot = 2 * order[first + k]
        both = jnp.concatenate(
            [weights[spot, 2 * FF :, :], weights[spot + 1, 2 * FF :, :]], axis=1
        )
        target[k] = jnp.dot(hid[...], both, preferred_element_type=F32).astype(BF)


def ffn_first_body(
    order, pack, gain, m0, m1, m2, m3, n0, n1, n2, n3, send, hid, weights, rows_x, sems
):
    def copies(sem, *spans):
        return [
            pltpu.make_async_copy(
                pack.at[:, pl.ds(at, size), :], weights.at[:, pl.ds(at, size), :], sems.at[sem]
            )
            for at, size in spans
        ]

    halves = ((0, 512), (512, FF - 512))
    parts = [
        copies(i, (at, width), (FF + at, width)) for i, (at, width) in enumerate(halves)
    ]
    parts.append(copies(2, (2 * FF, FF)))
    for part in parts:
        for copy in part:
            copy.start()
    ffn_rows(order, gain, (m0, m1, m2, m3, n0, n1, n2, n3), rows_x)
    for part, (at, width) in zip(parts, halves):
        for copy in part:
            copy.wait()
        ffn_hidden(weights, rows_x, hid, at, width)
    for copy in parts[2]:
        copy.wait()
    project_down(order, 4, hid, weights, send)


def ffn_next_body(
    order, weights, gain, m0, m1, m2, m3, n0, n1, n2, n3, send, hid, rows_x
):
    ffn_rows(order, gain, (m0, m1, m2, m3, n0, n1, n2, n3), rows_x)
    ffn_hidden(weights, rows_x, hid, 0, FF)
    project_down(order, 4, hid, weights, send)


def ffn_kernel(order, weights, gain, pieces, first):
    count = pieces[0].shape[0]
    shapes = (sds((4, count, COL), BF), sds((count, FF), BF))
    scratch = [pltpu.VMEM((count, D), BF)]
    if first:
        shapes += (sds((16, PACK, 128), BF),)
        scratch.append(pltpu.SemaphoreType.DMA((3,)))
        (weights,) = in_hbm(weights)
    return pl.pallas_call(
        ffn_first_body if first else ffn_next_body,
        out_shape=shapes,
        in_specs=[SMEM, HBM if first else VMEM] + [VMEM] * (len(pieces) + 1),
        out_specs=(VMEM,) * len(shapes),
        scratch_shapes=scratch,
        compiler_params=params(14),
        cost_estimate=pl.CostEstimate(flops=9_000_000_000, transcendentals=0, bytes_accessed=12_000_000),
        name="ffn",
    )(order, weights, gain, *pieces)


def keep_down_body(order, hid, weights, target):
    project_down(order, 0, hid, weights, target)


def keep_down_kernel(order, hid, weights):
    return pl.pallas_call(
        keep_down_body,
        out_shape=sds((4, hid.shape[0], COL), BF),
        in_specs=[SMEM, VMEM, VMEM],
        out_specs=VMEM,
        compiler_params=params(8),
        cost_estimate=pl.CostEstimate(flops=1_000_000_000, transcendentals=0, bytes_accessed=6_000_000),
        name="keep_down",
    )(order, hid, weights)


def turn(array, axis, distance):
    count = lax.axis_size(axis)
    return lax.ppermute(array, axis, [(i, (i + distance) % count) for i in range(count)])


def swap(array):
    return lax.ppermute(array, "c", [(0, 1), (1, 0)])


def reduce_chips(parts):
    c0, c1, c2, c3 = parts
    far = turn(c2, "x", 2)
    return c0, far, turn(c1, "x", 1), turn(c3, "x", -1)


def gather_chips(own):
    far = turn(own, "x", 2)
    return own, turn(own, "x", -1), far, turn(own, "x", 1)


def exchange(payload, axis):
    far = turn(payload, axis, 2)
    return [payload, turn(payload, axis, 1), far, turn(payload, axis, 3)]


def shards(
    arriving, content, gate, linked, raw, spike, taps_c, taps_p, shift, fading, skip,
    cluster_gain, blender, norm_gain, w_gate, w_up, w_down,
):
    x, c = lax.axis_index("x"), lax.axis_index("c")
    y, z = lax.axis_index("y"), lax.axis_index("z")
    chips = (x + jnp.arange(4, dtype=jnp.int32)) % 4
    order = jnp.concatenate([chips * 2 + c, chips * 2 + (1 - c)]).astype(jnp.int32)
    first_col = (2 * x + c).reshape(1)
    y, z = y.reshape(1), z.reshape(1)
    pack, tail, cum, tot, step, factors, ends, total, skip, taps_c, taps_p = head_kernel(
        w_gate.T, w_up.T, w_down, raw.T, spike.T, shift.reshape(1, HEADS),
        fading.reshape(1, HEADS), skip.reshape(1, HEADS), taps_c, taps_p.reshape(4, 2, ST),
        content, linked.reshape(T, 2, ST),
    )
    pack, tail, order, first_col, y, z, linked = lax.optimization_barrier(
        (pack, tail, order, first_col, y, z, linked)
    )
    gathered = lax.all_gather(pack, SP, axis=0, tiled=True).reshape(16, PACK, 128)
    pairs = linked.reshape(T, 256)
    halo = lax.ppermute(tail, SP, [(i, i + 1) for i in range(15)])
    values, maps, entering, payload = state_kernel(
        content, pairs, halo, factors, ends, total, taps_c, taps_p
    )
    line = exchange(payload, "y")
    local, opened = local_kernel(
        values, maps, cum, step, entering, skip, gate, blender
    )
    mine_cols = cols_kernel(first_col, arriving)
    payload_z, prefix, ahead = line_kernel(y, line)
    lines = exchange(payload_z, "z")
    incoming = incoming_kernel(z, lines, prefix, ahead)
    gain = norm_gain.reshape(1, D)
    mix_args = (incoming, local, maps, tot, opened, cluster_gain.reshape(1, CH), blender)
    (at_a, rows_a), (at_b, rows_b) = (0, FIRST), (FIRST, SECOND)
    send_a, mixed_a = mix_kernel(at_a, rows_a, order, *mix_args)
    got_a = swap(send_a)
    keep_a = keep_kernel(order, mixed_a, blender)
    parts = pair_kernel(keep_a, got_a)
    parts = reduce_chips(parts)
    own_a = own_kernel(at_a, parts, mine_cols)
    mine_a = gather_chips(own_a)
    send_b, mixed_b = mix_kernel(at_b, rows_b, order, *mix_args)
    got_b = swap(send_b)
    keep_b = keep_kernel(order, mixed_b, blender)
    parts = pair_kernel(keep_b, got_b)
    parts = reduce_chips(parts)
    own_b = own_kernel(at_b, parts, mine_cols)
    mine_b = gather_chips(own_b)
    theirs_a = tuple(swap(piece) for piece in mine_a)
    send, hid, weights = ffn_kernel(order, gathered, gain, (*mine_a, *theirs_a), True)
    got = swap(send)
    keep = keep_down_kernel(order, hid, weights)
    parts = pair_kernel(keep, got)
    last_a = reduce_chips(parts)
    theirs_b = tuple(swap(piece) for piece in mine_b)
    send, hid = ffn_kernel(order, weights, gain, (*mine_b, *theirs_b), False)
    got = swap(send)
    keep = keep_down_kernel(order, hid, weights)
    parts = pair_kernel(keep, got)
    last_b = reduce_chips(parts)
    return join_kernel(last_kernel(own_a, last_a), own_b, last_b)


def solution(mesh):
    torus = Mesh(mesh.devices.reshape(4, 4, 4, 2), ("z", "y", "x", "c"))
    tp = ("x", "c")
    return jax.shard_map(
        shards,
        mesh=torus,
        in_specs=(
            P(SP, None), P(SP, tp), P(SP, tp), P(SP, tp, None, None), P(SP, tp), P(SP, tp),
            P(None, tp), P(None, tp, None, None), P(tp), P(tp), P(tp), P(tp), P(tp, None),
            P(), P(SP, tp), P(SP, tp), P(tp, SP),
        ),
        out_specs=P(SP, tp),
        check_vma=False,
    )
```

```python
import functools

import jax
import jax.numpy as jnp
from jax import lax
from jax.experimental import pallas as pl
from jax.experimental.pallas import tpu as pltpu
from jax.sharding import Mesh
from jax.sharding import PartitionSpec as P


BF = jnp.bfloat16
F32 = jnp.float32
EPS = 1e-06
T = 1024
BLK = 128
NB = T // BLK
HEADS = 8
CH = 512
ST = 128
PAIR = 128
HALO = 16
LOGROWS = 8
D = 2048
COL = 256
FF = 704
PACK = 2 * FF + FF
FIRST = 512
SECOND = T - FIRST

SP = ("z", "y")

VMEM = pl.BlockSpec(memory_space=pltpu.VMEM)
SMEM = pl.BlockSpec(memory_space=pltpu.SMEM)
HBM = pl.BlockSpec(memory_space=pltpu.HBM)


def sds(shape, kind):
    return jax.ShapeDtypeStruct(shape, kind)


def params(mib=48):
    return pltpu.CompilerParams(vmem_limit_bytes=mib * 1024 * 1024)


def silu(x):
    return x * jax.nn.sigmoid(x)


def hi_dot(a, b):
    return jnp.dot(a, b, preferred_element_type=F32, precision=lax.Precision.HIGHEST)


def lane_low():
    return lax.broadcasted_iota(jnp.int32, (1, PAIR), 1) < PAIR // 2


def spread(rows, width, pieces):
    parts, rest = [], rows
    for _ in range(pieces):
        part = rest.astype(BF)
        rest = rest - part.astype(F32)
        parts.append(part)
    head = lax.broadcasted_iota(jnp.int32, (HEADS, HEADS * width), 0)
    lane = lax.broadcasted_iota(jnp.int32, (HEADS, HEADS * width), 1)
    ones = ((lane >= head * width) & (lane < (head + 1) * width)).astype(F32).astype(BF)
    return lax.dot_general(
        jnp.concatenate(parts, axis=0), jnp.concatenate([ones] * pieces, axis=0),
        (((0,), (0,)), ((), ())), preferred_element_type=F32,
    )


def block_lanes(b):
    return pl.ds(pl.multiple_of(b * BLK, BLK), BLK)


def conv_rows(ext, taps):
    total = ext[HALO - 3 : HALO - 3 + BLK] * taps[0:1]
    for k in range(1, 4):
        total = total + ext[HALO - 3 + k : HALO - 3 + k + BLK] * taps[k : k + 1]
    return silu(total).astype(BF)


def column(row):
    own = lax.broadcasted_iota(jnp.int32, (HEADS, HEADS), 0) == lax.broadcasted_iota(
        jnp.int32, (HEADS, HEADS), 1
    )
    spread_row = jnp.broadcast_to(row, (HEADS, HEADS))
    return jnp.sum(jnp.where(own, spread_row, 0.0), axis=1, keepdims=True)


def in_hbm(*arrays):
    return tuple(pltpu.with_memory_space_constraint(a, pltpu.HBM) for a in arrays)


def softplus(x):
    return jnp.maximum(x, 0.0) + jnp.log1p(jnp.exp(-jnp.abs(x)))


def head_body(
    gate, up, down, raw_in, spike_in, shift_in, fading_in, skip_in, taps_c_in, taps_p_in,
    content_in, pairs_in,
    pack, tail, cum_out, tot_out, step_out, factors, ends, total_out, skip_out, taps_c_out,
    taps_p_out,
    packed, raw, spike, shift, fading, skip, taps_c, taps_p, content, pairs, sems,
):
    weights = [
        pltpu.make_async_copy(part, packed.at[pl.ds(i * FF, FF), :], sems.at[0])
        for i, part in enumerate((gate, up, down))
    ]
    small = [
        pltpu.make_async_copy(source, target, sems.at[1])
        for source, target in (
            (raw_in, raw), (spike_in, spike), (shift_in, shift), (fading_in, fading),
            (skip_in, skip), (taps_c_in, taps_c), (taps_p_in, taps_p),
            (content_in.at[pl.ds(T - HALO, HALO), :], content),
            (pairs_in.at[pl.ds(T - HALO, HALO)], pairs),
        )
    ]
    for copy in weights + small:
        copy.start()
    for copy in weights:
        copy.wait()
    out = pltpu.make_async_copy(packed, pack, sems.at[2])
    out.start()
    for copy in small:
        copy.wait()
    tail[:, 0:CH] = content[...]
    rows = pairs[...].astype(F32)
    tail[:, CH : CH + ST] = rows[:, 0, :].astype(BF)
    tail[:, CH + ST : CH + 2 * ST] = rows[:, 1, :].astype(BF)
    row = lax.broadcasted_iota(jnp.int32, (BLK, BLK), 0)
    col = lax.broadcasted_iota(jnp.int32, (BLK, BLK), 1)
    triu = (row <= col).astype(F32)
    step = softplus(raw[...].astype(F32) + column(shift[...]))
    step_out[...] = step
    log = -jnp.exp(column(fading[...])) * step + spike[...]
    cum = hi_dot(
        jnp.concatenate([log[:, b * BLK : (b + 1) * BLK] for b in range(NB)], axis=0), triu
    )
    prior = jnp.zeros((HEADS, 1), F32)
    for b in range(NB):
        lanes = slice(b * BLK, (b + 1) * BLK)
        here = cum[b * HEADS : (b + 1) * HEADS]
        end = here[:, BLK - 1 : BLK]
        cum_out[:, lanes] = here
        tot_out[:, lanes] = here + prior
        factors[b] = step[:, lanes] * jnp.exp(end - here)
        ends[b] = jnp.broadcast_to(jnp.exp(end), (HEADS, BLK))
        prior = prior + end
    total_out[...] = spread(jnp.broadcast_to(prior, (HEADS, BLK)), 64, 3)[0:8]
    skip_out[...] = spread(jnp.broadcast_to(column(skip[...]), (HEADS, BLK)), 64, 3)[0:8]
    taps_c_out[0:4, :] = taps_c[...].astype(F32)
    wide = taps_p[...].astype(F32)
    taps_p_out[0:4, 0:ST] = wide[:, 0, :]
    taps_p_out[0:4, ST : 2 * ST] = wide[:, 1, :]
    out.wait()


def head_kernel(*args):
    small = args[3:10]
    return pl.pallas_call(
        head_body,
        out_shape=(
            sds((PACK, 128), BF),
            sds((HALO, CH + 256), BF),
            sds((HEADS, T), F32),
            sds((HEADS, T), F32),
            sds((HEADS, T), F32),
            sds((NB, HEADS, BLK), F32),
            sds((NB, HEADS, BLK), F32),
            sds((8, CH), F32),
            sds((8, CH), F32),
            sds((8, CH), F32),
            sds((8, 256), F32),
        ),
        in_specs=[HBM] * len(args),
        out_specs=(HBM,) + (VMEM,) * 10,
        scratch_shapes=[pltpu.VMEM((PACK, 128), BF)]
        + [pltpu.VMEM(a.shape, a.dtype) for a in small]
        + [
            pltpu.VMEM((HALO, CH), BF),
            pltpu.VMEM((HALO, 2, ST), BF),
            pltpu.SemaphoreType.DMA((3,)),
        ],
        compiler_params=params(8),
        name="head",
    )(*in_hbm(*args))


def state_body(
    content, pairs, halo, factors, ends, total, taps_c, taps_p,
    values, maps, entering, payload,
    ext_c, ext_p, carry,
):
    ext_c[0:HALO] = halo[:, 0:CH]
    ext_p[0:HALO] = halo[:, CH : CH + 256]
    ext_c[HALO : HALO + T] = content[...]
    ext_p[HALO : HALO + T] = pairs[...]
    carry[...] = jnp.zeros((ST, CH), F32)
    tc = taps_c[...]
    tp = taps_p[...]

    def block(b, _):
        at = pl.multiple_of(b * BLK, BLK)
        rows = pl.ds(at, BLK)
        wide = pl.ds(at, BLK + HALO)
        v = conv_rows(ext_c[wide, :].astype(F32), tc)
        m = conv_rows(ext_p[wide, :].astype(F32), tp)
        values[rows, :] = v
        maps[rows, :] = m
        scaled = (v.astype(F32) * spread(factors[b], 64, 2)).astype(BF)
        added = lax.dot_general(
            m[:, 0:ST], scaled, (((0,), (0,)), ((), ())), preferred_element_type=F32
        )
        old = carry[...]
        entering[b] = old.astype(BF)
        carry[...] = old * spread(ends[b], 64, 2) + added
        return 0

    lax.fori_loop(0, NB, block, 0, unroll=8)
    payload[0:ST, :] = carry[...].astype(BF)
    high = total[...].astype(BF)
    low = (total[...] - high.astype(F32)).astype(BF)
    payload[ST : ST + LOGROWS, :] = jnp.concatenate([high[0:4], low[0:4]], axis=0)


def state_kernel(*args):
    return pl.pallas_call(
        state_body,
        out_shape=(
            sds((T, CH), BF),
            sds((T, 256), BF),
            sds((NB, ST, CH), BF),
            sds((ST + LOGROWS, CH), BF),
        ),
        in_specs=[VMEM] * 8,
        out_specs=(VMEM,) * 4,
        scratch_shapes=[
            pltpu.VMEM((T + HALO, CH), BF),
            pltpu.VMEM((T + HALO, 256), BF),
            pltpu.VMEM((ST, CH), F32),
        ],
        compiler_params=params(12),
        name="state",
    )(*args)


def local_body(values, maps, cum_in, step_in, entering, skip, gate, blend, out, gate_out):
    row = lax.broadcasted_iota(jnp.int32, (BLK, BLK), 0)
    col = lax.broadcasted_iota(jnp.int32, (BLK, BLK), 1)
    causal = col <= row
    low = lane_low()
    gain = skip[0:1, :]

    def block(b, _):
        rows = block_lanes(b)
        v = values[rows, :]
        m = maps[rows, :]
        write, read = m[:, 0:ST], m[:, ST : 2 * ST]
        cum = cum_in[:, rows]
        cum_wide = spread(cum, BLK, 3)
        steps = step_in[:, rows]
        meet = lax.dot_general(
            read, write, (((1,), (1,)), ((), ())), preferred_element_type=F32
        )
        parts = []
        for p in range(HEADS // 2):
            weights = []
            for h in (2 * p, 2 * p + 1):
                gap = cum_wide[:, h * BLK : (h + 1) * BLK] - cum[h : h + 1, :]
                decay = jnp.exp(jnp.where(causal, gap, -jnp.inf))
                weights.append((meet * decay * steps[h : h + 1, :]).astype(BF))
            vp = v[:, p * PAIR : (p + 1) * PAIR]
            none = jnp.zeros_like(vp)
            stacked = jnp.concatenate(
                [jnp.where(low, vp, none), jnp.where(low, none, vp)], axis=0
            )
            parts.append(
                jnp.dot(
                    jnp.concatenate(weights, axis=1), stacked, preferred_element_type=F32
                )
            )
        within = jnp.concatenate(parts, axis=1)
        carried = jnp.dot(read, entering[b], preferred_element_type=F32)
        carried = carried * spread(jnp.exp(cum), 64, 2)
        out[rows, :] = within + carried + v.astype(F32) * gain
        gate_out[rows, :] = silu(gate[rows, :].astype(F32))
        return 0

    lax.fori_loop(0, NB, block, 0)


def local_kernel(*args):
    return pl.pallas_call(
        local_body,
        out_shape=(sds((T, CH), F32), sds((T, CH), F32)),
        in_specs=[VMEM] * 8,
        out_specs=(VMEM,) * 2,
        compiler_params=params(12),
        cost_estimate=pl.CostEstimate(flops=6_000_000_000, transcendentals=0, bytes_accessed=6_000_000),
        name="local",
    )(*args)


def log_row(ref):
    return ref[ST : ST + 1, :].astype(F32) + ref[ST + 4 : ST + 5, :].astype(F32)


def scan_line(place, refs, state, prefix):
    state[...] = jnp.zeros((ST, CH), F32)
    prefix[...] = jnp.zeros((ST, CH), F32)
    count = len(refs)
    logs = [log_row(r) for r in refs]
    whole = jnp.zeros((1, CH), F32)
    ahead = jnp.zeros((1, CH), F32)
    for j in range(count):
        for d in range(count):

            @pl.when(lax.rem(place - j + count, count) == d)
            def _(d=d):
                if d == 0:
                    prefix[...] = state[...]
                state[...] = state[...] * jnp.exp(logs[d]) + refs[d][0:ST, :].astype(F32)

    for d in range(count):
        whole = whole + logs[d]
        ahead = ahead + jnp.where(place >= d, logs[d], 0.0) if d else ahead
    return whole, ahead


def line_body(place, r0, r1, r2, r3, payload, prefix, ahead_out, state):
    whole, ahead = scan_line(place[0], (r0, r1, r2, r3), state, prefix)
    payload[0:ST, :] = state[...].astype(BF)
    high = whole.astype(BF)
    low = (whole - high.astype(F32)).astype(BF)
    payload[ST : ST + LOGROWS, :] = jnp.concatenate(
        [jnp.broadcast_to(high, (4, CH)), jnp.broadcast_to(low, (4, CH))], axis=0
    )
    ahead_out[...] = jnp.broadcast_to(ahead, (8, CH))


def line_kernel(place, received):
    return pl.pallas_call(
        line_body,
        out_shape=(
            sds((ST + LOGROWS, CH), BF),
            sds((ST, CH), F32),
            sds((8, CH), F32),
        ),
        in_specs=[SMEM] + [VMEM] * 4,
        out_specs=(VMEM,) * 3,
        scratch_shapes=[pltpu.VMEM((ST, CH), F32)],
        compiler_params=params(8),
        name="line",
    )(place, *received)


def incoming_body(place, q0, q1, q2, q3, prefix, ahead, incoming, state, prefix_z):
    scan_line(place[0], (q0, q1, q2, q3), state, prefix_z)
    incoming[...] = (prefix_z[...] * jnp.exp(ahead[0:1, :]) + prefix[...]).astype(BF)


def incoming_kernel(place, received, prefix, ahead):
    return pl.pallas_call(
        incoming_body,
        out_shape=sds((ST, CH), BF),
        in_specs=[SMEM] + [VMEM] * 6,
        out_specs=VMEM,
        scratch_shapes=[pltpu.VMEM((ST, CH), F32), pltpu.VMEM((ST, CH), F32)],
        compiler_params=params(8),
        name="incoming",
    )(place, *received, prefix, ahead)


def mix_body(
    start, count, order, incoming, local, maps, tot, gate, gain, blend, send, mixed
):
    rescale = gain[...]

    def block(b, _):
        rows = pl.ds(pl.multiple_of(start + b * BLK, BLK), BLK)
        read = maps[rows, ST : 2 * ST]
        arrived = jnp.dot(read, incoming[...], preferred_element_type=F32)
        mixer = local[rows, :] + arrived * spread(jnp.exp(tot[:, rows]), 64, 2)
        gated = mixer * gate[rows, :]
        scale = lax.rsqrt(jnp.mean(gated * gated, axis=1, keepdims=True) + EPS)
        mixed[pl.ds(pl.multiple_of(b * BLK, BLK), BLK), :] = (gated * scale * rescale).astype(BF)
        return 0

    lax.fori_loop(0, count // BLK, block, 0, unroll=4)
    project(order, 4, mixed, blend, send)


def project(order, first, rows, weights, target):
    for k in range(4):
        cols = pl.ds(pl.multiple_of(order[first + k] * COL, COL), COL)
        target[k] = jnp.dot(
            rows[...], weights[:, cols], preferred_element_type=F32
        ).astype(BF)


def cols_body(col, arriving, out):
    out[...] = arriving[...]


def cols_kernel(col, arriving):
    return pl.pallas_call(
        cols_body,
        out_shape=sds((T, COL), BF),
        grid_spec=pltpu.PrefetchScalarGridSpec(
            num_scalar_prefetch=1,
            grid=(1,),
            in_specs=[pl.BlockSpec((T, COL), lambda _, col: (0, col[0]))],
            out_specs=VMEM,
        ),
        compiler_params=params(4),
        name="cols",
    )(col, *in_hbm(arriving))


def keep_body(order, rows, weights, target):
    project(order, 0, rows, weights, target)


def keep_kernel(order, rows, weights):
    return pl.pallas_call(
        keep_body,
        out_shape=sds((4, rows.shape[0], COL), BF),
        in_specs=[SMEM, VMEM, VMEM],
        out_specs=VMEM,
        compiler_params=params(8),
        cost_estimate=pl.CostEstimate(flops=1_000_000_000, transcendentals=0, bytes_accessed=6_000_000),
        name="keep",
    )(order, rows, weights)


def mix_kernel(start, count, order, *args):
    return pl.pallas_call(
        functools.partial(mix_body, start, count),
        out_shape=(sds((4, count, COL), BF), sds((count, CH), BF)),
        in_specs=[SMEM] + [VMEM] * 7,
        out_specs=(VMEM,) * 2,
        compiler_params=params(8),
        cost_estimate=pl.CostEstimate(flops=3_000_000_000, transcendentals=0, bytes_accessed=6_000_000),
        name="mix",
    )(order, *args)


def pair_body(keep, got, c0, c1, c2, c3):
    for k, out in enumerate((c0, c1, c2, c3)):
        out[...] = (keep[k].astype(F32) + got[k].astype(F32)).astype(BF)


def pair_kernel(keep, got):
    count = keep.shape[1]
    return pl.pallas_call(
        pair_body,
        out_shape=(sds((count, COL), BF),) * 4,
        in_specs=[VMEM] * 2,
        out_specs=(VMEM,) * 4,
        compiler_params=params(8),
        name="pair",
    )(keep, got)


def total_of(refs):
    total = refs[0][...].astype(F32)
    for r in refs[1:]:
        total = total + r[...].astype(F32)
    return total


def own_body(start, c0, f1, f2, f3, arriving, out):
    count = out.shape[0]
    base = arriving[start : start + count, :].astype(F32)
    out[...] = (base + total_of((c0, f1, f2, f3))).astype(BF)


def own_kernel(start, parts, arriving):
    count = parts[0].shape[0]
    return pl.pallas_call(
        functools.partial(own_body, start),
        out_shape=sds((count, COL), BF),
        in_specs=[VMEM] * 5,
        out_specs=VMEM,
        compiler_params=params(8),
        name="own",
    )(*parts, arriving)


def last_body(own, c0, f1, f2, f3, out):
    out[...] = (own[...].astype(F32) + 0.5 * total_of((c0, f1, f2, f3))).astype(BF)


def last_kernel(own, parts):
    return pl.pallas_call(
        last_body,
        out_shape=sds(own.shape, BF),
        in_specs=[VMEM] * 5,
        out_specs=VMEM,
        compiler_params=params(8),
        name="last",
    )(own, *parts)


def join_body(first, own, c0, f1, f2, f3, out):
    split = first.shape[0]
    out[:split, :] = first[...]
    out[split:, :] = (own[...].astype(F32) + 0.5 * total_of((c0, f1, f2, f3))).astype(BF)


def join_kernel(first, own, parts):
    return pl.pallas_call(
        join_body,
        out_shape=sds((T, COL), BF),
        in_specs=[VMEM] * 6,
        out_specs=VMEM,
        compiler_params=params(8),
        name="join",
    )(first, own, *parts)


NORM_ROWS = 128


def row_scale(pieces):
    total = None
    for x in pieces:
        for at in range(0, x.shape[1], 128):
            part = x[:, at : at + 128]
            total = part * part if total is None else total + part * part
    return lax.rsqrt(jnp.sum(total, axis=1, keepdims=True) * (1.0 / D) + EPS)


def ffn_rows(order, gain, refs, rows_x):
    def norm(b, _):
        rows = pl.ds(pl.multiple_of(b * NORM_ROWS, NORM_ROWS), NORM_ROWS)
        scale = row_scale([r[rows, :].astype(F32) for r in refs])
        for i, r in enumerate(refs):
            cols = pl.ds(pl.multiple_of(order[i] * COL, COL), COL)
            rows_x[rows, cols] = (r[rows, :].astype(F32) * scale * gain[:, cols]).astype(BF)
        return 0

    lax.fori_loop(0, rows_x.shape[0] // NORM_ROWS, norm, 0, unroll=2)


def ffn_hidden(weights, rows_x, hid, at, width):
    over_k = (((1,), (1,)), ((), ()))

    def columns(at):
        return jnp.concatenate([weights[j, at : at + width, :] for j in range(16)], axis=1)

    gate = lax.dot_general(rows_x[...], columns(at), over_k, preferred_element_type=F32)
    up = lax.dot_general(rows_x[...], columns(FF + at), over_k, preferred_element_type=F32)
    hid[:, at : at + width] = (silu(gate) * up).astype(BF)


def project_down(order, first, hid, weights, target):
    for k in range(4):
        spot = 2 * order[first + k]
        both = jnp.concatenate(
            [weights[spot, 2 * FF :, :], weights[spot + 1, 2 * FF :, :]], axis=1
        )
        target[k] = jnp.dot(hid[...], both, preferred_element_type=F32).astype(BF)


def ffn_first_body(
    order, pack, gain, m0, m1, m2, m3, n0, n1, n2, n3, send, hid, weights, rows_x, sems
):
    def copies(sem, *spans):
        return [
            pltpu.make_async_copy(
                pack.at[:, pl.ds(at, size), :], weights.at[:, pl.ds(at, size), :], sems.at[sem]
            )
            for at, size in spans
        ]

    halves = ((0, 512), (512, FF - 512))
    parts = [
        copies(i, (at, width), (FF + at, width)) for i, (at, width) in enumerate(halves)
    ]
    parts.append(copies(2, (2 * FF, FF)))
    for part in parts:
        for copy in part:
            copy.start()
    ffn_rows(order, gain, (m0, m1, m2, m3, n0, n1, n2, n3), rows_x)
    for part, (at, width) in zip(parts, halves):
        for copy in part:
            copy.wait()
        ffn_hidden(weights, rows_x, hid, at, width)
    for copy in parts[2]:
        copy.wait()
    project_down(order, 4, hid, weights, send)


def ffn_next_body(
    order, weights, gain, m0, m1, m2, m3, n0, n1, n2, n3, send, hid, rows_x
):
    ffn_rows(order, gain, (m0, m1, m2, m3, n0, n1, n2, n3), rows_x)
    ffn_hidden(weights, rows_x, hid, 0, FF)
    project_down(order, 4, hid, weights, send)


def ffn_kernel(order, weights, gain, pieces, first):
    count = pieces[0].shape[0]
    shapes = (sds((4, count, COL), BF), sds((count, FF), BF))
    scratch = [pltpu.VMEM((count, D), BF)]
    if first:
        shapes += (sds((16, PACK, 128), BF),)
        scratch.append(pltpu.SemaphoreType.DMA((3,)))
        (weights,) = in_hbm(weights)
    return pl.pallas_call(
        ffn_first_body if first else ffn_next_body,
        out_shape=shapes,
        in_specs=[SMEM, HBM if first else VMEM] + [VMEM] * (len(pieces) + 1),
        out_specs=(VMEM,) * len(shapes),
        scratch_shapes=scratch,
        compiler_params=params(14),
        cost_estimate=pl.CostEstimate(flops=9_000_000_000, transcendentals=0, bytes_accessed=12_000_000),
        name="ffn",
    )(order, weights, gain, *pieces)


def keep_down_body(order, hid, weights, target):
    project_down(order, 0, hid, weights, target)


def keep_down_kernel(order, hid, weights):
    return pl.pallas_call(
        keep_down_body,
        out_shape=sds((4, hid.shape[0], COL), BF),
        in_specs=[SMEM, VMEM, VMEM],
        out_specs=VMEM,
        compiler_params=params(8),
        cost_estimate=pl.CostEstimate(flops=1_000_000_000, transcendentals=0, bytes_accessed=6_000_000),
        name="keep_down",
    )(order, hid, weights)


def turn(array, axis, distance):
    count = lax.axis_size(axis)
    return lax.ppermute(array, axis, [(i, (i + distance) % count) for i in range(count)])


def swap(array):
    return lax.ppermute(array, "c", [(0, 1), (1, 0)])


def reduce_chips(parts):
    c0, c1, c2, c3 = parts
    far = turn(c2, "x", 2)
    return c0, far, turn(c1, "x", 1), turn(c3, "x", -1)


def gather_chips(own):
    far = turn(own, "x", 2)
    return own, turn(own, "x", -1), far, turn(own, "x", 1)


def exchange(payload, axis):
    far = turn(payload, axis, 2)
    return [payload, turn(payload, axis, 1), far, turn(payload, axis, 3)]


def shards(
    arriving, content, gate, linked, raw, spike, taps_c, taps_p, shift, fading, skip,
    cluster_gain, blender, norm_gain, w_gate, w_up, w_down,
):
    x, c = lax.axis_index("x"), lax.axis_index("c")
    y, z = lax.axis_index("y"), lax.axis_index("z")
    chips = (x + jnp.arange(4, dtype=jnp.int32)) % 4
    order = jnp.concatenate([chips * 2 + c, chips * 2 + (1 - c)]).astype(jnp.int32)
    first_col = (2 * x + c).reshape(1)
    y, z = y.reshape(1), z.reshape(1)
    pack, tail, cum, tot, step, factors, ends, total, skip, taps_c, taps_p = head_kernel(
        w_gate.T, w_up.T, w_down, raw.T, spike.T, shift.reshape(1, HEADS),
        fading.reshape(1, HEADS), skip.reshape(1, HEADS), taps_c, taps_p.reshape(4, 2, ST),
        content, linked.reshape(T, 2, ST),
    )
    pack, tail, order, first_col, y, z, linked = lax.optimization_barrier(
        (pack, tail, order, first_col, y, z, linked)
    )
    gathered = lax.all_gather(pack, SP, axis=0, tiled=True).reshape(16, PACK, 128)
    pairs = linked.reshape(T, 256)
    halo = lax.ppermute(tail, SP, [(i, i + 1) for i in range(15)])
    values, maps, entering, payload = state_kernel(
        content, pairs, halo, factors, ends, total, taps_c, taps_p
    )
    line = exchange(payload, "y")
    local, opened = local_kernel(
        values, maps, cum, step, entering, skip, gate, blender
    )
    mine_cols = cols_kernel(first_col, arriving)
    payload_z, prefix, ahead = line_kernel(y, line)
    lines = exchange(payload_z, "z")
    incoming = incoming_kernel(z, lines, prefix, ahead)
    gain = norm_gain.reshape(1, D)
    mix_args = (incoming, local, maps, tot, opened, cluster_gain.reshape(1, CH), blender)
    (at_a, rows_a), (at_b, rows_b) = (0, FIRST), (FIRST, SECOND)
    send_a, mixed_a = mix_kernel(at_a, rows_a, order, *mix_args)
    got_a = swap(send_a)
    keep_a = keep_kernel(order, mixed_a, blender)
    parts = pair_kernel(keep_a, got_a)
    parts = reduce_chips(parts)
    own_a = own_kernel(at_a, parts, mine_cols)
    mine_a = gather_chips(own_a)
    send_b, mixed_b = mix_kernel(at_b, rows_b, order, *mix_args)
    got_b = swap(send_b)
    keep_b = keep_kernel(order, mixed_b, blender)
    parts = pair_kernel(keep_b, got_b)
    parts = reduce_chips(parts)
    own_b = own_kernel(at_b, parts, mine_cols)
    mine_b = gather_chips(own_b)
    theirs_a = tuple(swap(piece) for piece in mine_a)
    send, hid, weights = ffn_kernel(order, gathered, gain, (*mine_a, *theirs_a), True)
    got = swap(send)
    keep = keep_down_kernel(order, hid, weights)
    parts = pair_kernel(keep, got)
    last_a = reduce_chips(parts)
    theirs_b = tuple(swap(piece) for piece in mine_b)
    send, hid = ffn_kernel(order, weights, gain, (*mine_b, *theirs_b), False)
    got = swap(send)
    keep = keep_down_kernel(order, hid, weights)
    parts = pair_kernel(keep, got)
    last_b = reduce_chips(parts)
    return join_kernel(last_kernel(own_a, last_a), own_b, last_b)


def solution(mesh):
    torus = Mesh(mesh.devices.reshape(4, 4, 4, 2), ("z", "y", "x", "c"))
    tp = ("x", "c")
    return jax.shard_map(
        shards,
        mesh=torus,
        in_specs=(
            P(SP, None), P(SP, tp), P(SP, tp), P(SP, tp, None, None), P(SP, tp), P(SP, tp),
            P(None, tp), P(None, tp, None, None), P(tp), P(tp), P(tp), P(tp), P(tp, None),
            P(), P(SP, tp), P(SP, tp), P(tp, SP),
        ),
        out_specs=P(SP, tp),
        check_vma=False,
    )
```
